32 devices in a mesh: kv: 8 (over z, x), tp: 4 (over y, core).
Axes of the slice: x: 2, y: 2, z: 4, core: 2. Of those that a mesh axis runs over, the one named last changes fastest.
Arguments:
- stream: bfloat16 [128, 4096], P(None, ('kv', 'tp')), may hold values from -20 to 20
- ssm_state: float32 [128, 64, 64, 128], P('kv', 'tp'), may hold values from -1.8 to 1.8
- conv_state: bfloat16 [128, 3, 8, 768], P('kv', None, 'tp'), may hold values from -6 to 6
- first_gain: float32 [4096], P(('kv', 'tp')), may hold values from 0.1 to 1.9
- first_gate: bfloat16 [4096, 11264], P('kv', 'tp'), may hold values from -0.09375 to 0.09375
- first_up: bfloat16 [4096, 11264], P('kv', 'tp'), may hold values from -0.09375 to 0.09375
- first_down: bfloat16 [11264, 4096], P('tp', 'kv'), may hold values from -0.0546875 to 0.0546875
- mix_gain: float32 [4096], P(('kv', 'tp')), may hold values from 0.1 to 1.9
- gate_in: bfloat16 [4096, 4096], P('kv', 'tp'), may hold values from -0.09375 to 0.09375
- value_in: bfloat16 [4096, 4096], P('kv', 'tp'), may hold values from -0.09375 to 0.09375
- write_in: bfloat16 [4096, 1024], P('kv', 'tp'), may hold values from -0.09375 to 0.09375
- read_in: bfloat16 [4096, 1024], P('kv', 'tp'), may hold values from -0.09375 to 0.09375
- step_in: bfloat16 [4096, 64], P('kv', 'tp'), may hold values from -0.09375 to 0.09375
- conv_weight: float32 [4, 8, 768], P(None, 'tp'), may hold values from -3 to 3
- step_bias: float32 [64], P('tp'), may hold values from -3 to 0.5
- log_decay_rate: float32 [64], P('tp'), may hold values from -1 to 2.5
- group_gain: float32 [4096], P('tp'), may hold values from 0.1 to 1.9
- out_weight: bfloat16 [4096, 4096], P('tp', 'kv'), may hold values from -0.09375 to 0.09375
- last_norm_gain: float32 [4096], P(('kv', 'tp')), may hold values from 0.1 to 1.9
- second_gate: bfloat16 [4096, 11264], P('kv', 'tp'), may hold values from -0.09375 to 0.09375
- second_up: bfloat16 [4096, 11264], P('kv', 'tp'), may hold values from -0.09375 to 0.09375
- second_down: bfloat16 [11264, 4096], P('tp', 'kv'), may hold values from -0.109375 to 0.109375
Outputs:
- next_stream: bfloat16 [128, 4096], P(None, ('kv', 'tp'))
- ssm_next: float32 [128, 64, 64, 128], P('kv', 'tp')
- conv_next: bfloat16 [128, 3, 8, 768], P('kv', None, 'tp')
The draws below stay inside these ranges and needn't reach their ends.
All inputs are finite; a program needn't handle non-finite values.
Results may differ from the reference program's by a relative error of at most 0.015.
Values may be sent and summed in bfloat16 or wider, within the bound.
A program may use at most 128 MiB of HBM per device.

```python
import jax
import jax.numpy as jnp
from jax import lax

D = 4096
FF = 11264
HEADS = 64
HEAD_DIM = 64
STATE = 128
GROUPS = 8
TAPS = 4
SEQS = 128
GROUP_CH = 768
N_KV = 8
N_TP = 4


def draw_stream(key, part):
    noise_key = jax.random.fold_in(jax.random.fold_in(key, 11), 0)
    shard_width = D // (N_KV * N_TP)
    column = jnp.arange(D, dtype=jnp.int32)
    tp_index = column // shard_width % N_TP
    kv_index = column // (shard_width * N_TP)
    tp_frac = tp_index.astype(jnp.float32) / max(N_TP - 1, 1)
    kv_frac = kv_index.astype(jnp.float32) / max(N_KV - 1, 1)
    column_scale = jnp.exp(jnp.log(0.3) + jnp.log(10.0) * tp_frac + jnp.log(1.3) * kv_frac)[None]
    base = jax.random.truncated_normal(noise_key, -4.0, 4.0, (SEQS, D), jnp.float32)
    return (base * column_scale).astype(jnp.bfloat16)


def level_of(rng, dims, cuts, least, high):
    def one(dim, blocks):
        steps = jax.random.uniform(jax.random.fold_in(jax.random.fold_in(rng, 6), dim), (blocks,), jnp.float32, least / len(cuts), high / len(cuts))
        return jnp.repeat(jnp.exp(steps), dims[dim] // blocks).reshape((-1,) + (1,) * (len(dims) - dim - 1))

    loudness = one(*cuts[0])
    for cut in cuts[1:]:
        loudness = loudness * one(*cut)
    return loudness


def scatter_about(key, dims, scale, limit, pieces=(), held_as=jnp.bfloat16):
    result = scale * jax.random.normal(key, dims, jnp.float32)
    if pieces:
        result = result * level_of(key, dims, pieces, -0.22, 0.18)
    return jnp.clip(result, -limit, limit).astype(held_as)


def setup_inputs(seed: int = 0) -> dict:
    seeds = jax.random.split(jax.random.key(seed), 23)
    stream = draw_stream(jax.random.fold_in(seeds[22], 71), 0)
    ssm_state = scatter_about(seeds[1], (SEQS, HEADS, HEAD_DIM, STATE), 0.3, 1.8, ((0, 8), (1, 4)), jnp.float32)
    conv_state = scatter_about(seeds[2], (SEQS, TAPS - 1, GROUPS, GROUP_CH), 1.0, 6.0, ((0, 8), (2, 4)))
    first_gain = jnp.clip(1.0 + 0.18 * jax.random.normal(seeds[3], (D,), jnp.float32), 0.1, 1.9)
    first_gate = scatter_about(seeds[4], (D, FF), D ** -0.5, 0.09375, ((0, 8), (1, 4)))
    first_up = scatter_about(seeds[5], (D, FF), D ** -0.5, 0.09375, ((0, 8), (1, 4)))
    first_down = scatter_about(seeds[6], (FF, D), FF ** -0.5, 0.0546875, ((0, 4), (1, 8)))
    mix_gain = jnp.clip(1.0 + 0.18 * jax.random.normal(seeds[7], (D,), jnp.float32), 0.1, 1.9)
    gate_in = scatter_about(seeds[8], (D, HEADS * HEAD_DIM), D ** -0.5, 0.09375, ((0, 8), (1, 4)))
    value_in = scatter_about(seeds[9], (D, HEADS * HEAD_DIM), D ** -0.5, 0.09375, ((0, 8), (1, 4)))
    write_in = scatter_about(seeds[10], (D, GROUPS * STATE), D ** -0.5, 0.09375, ((0, 8), (1, 4)))
    read_in = scatter_about(seeds[11], (D, GROUPS * STATE), D ** -0.5, 0.09375, ((0, 8), (1, 4)))
    step_in = scatter_about(seeds[12], (D, HEADS), D ** -0.5, 0.09375, ((0, 8), (1, 4)))
    conv_weight = scatter_about(seeds[13], (TAPS, GROUPS, GROUP_CH), TAPS ** -0.5, 3.0, ((1, 4),), jnp.float32)
    step_bias = jnp.clip(-3.0 + 3.5 * jax.random.uniform(seeds[14], (HEADS,), jnp.float32) ** level_of(seeds[14], (HEADS,), ((0, 4),), -0.2, 0.2), -3.0, 0.5)
    log_decay_rate = jnp.clip(-1.0 + 3.5 * jax.random.uniform(seeds[15], (HEADS,), jnp.float32) ** level_of(seeds[15], (HEADS,), ((0, 4),), -0.2, 0.2), -1.0, 2.5)
    group_gain = jnp.clip(1.0 + 0.18 * jax.random.normal(seeds[16], (HEADS * HEAD_DIM,), jnp.float32), 0.1, 1.9)
    out_weight = scatter_about(seeds[17], (HEADS * HEAD_DIM, D), (HEADS * HEAD_DIM) ** -0.5, 0.09375, ((0, 4), (1, 8)))
    last_norm_gain = jnp.clip(1.0 + 0.18 * jax.random.normal(seeds[18], (D,), jnp.float32), 0.1, 1.9)
    second_gate = scatter_about(seeds[19], (D, FF), D ** -0.5, 0.09375, ((0, 8), (1, 4)))
    second_up = scatter_about(seeds[20], (D, FF), D ** -0.5, 0.09375, ((0, 8), (1, 4)))
    second_down = scatter_about(seeds[21], (FF, D), (FF // 4) ** -0.5, 0.109375, ((0, 4), (1, 8)))
    return dict(stream=stream, ssm_state=ssm_state, conv_state=conv_state, first_gain=first_gain, first_gate=first_gate, first_up=first_up, first_down=first_down, mix_gain=mix_gain, gate_in=gate_in, value_in=value_in, write_in=write_in, read_in=read_in, step_in=step_in, conv_weight=conv_weight, step_bias=step_bias, log_decay_rate=log_decay_rate, group_gain=group_gain, out_weight=out_weight, last_norm_gain=last_norm_gain, second_gate=second_gate, second_up=second_up, second_down=second_down)


norm_epsilon = 1e-06

def norm_rows(stream, gain):
    values = stream.astype(jnp.float32)
    scaled = (values * gain.astype(jnp.float32)[None]).astype(jnp.bfloat16)
    factor = lax.rsqrt(lax.optimization_barrier(jnp.mean(values * values, axis=1, keepdims=True)) + norm_epsilon)
    return (scaled, factor)

def blockwise_down(hidden, weight_matrix):
    batch = hidden.shape[0]
    block_list = hidden.reshape(batch, N_TP, -1).astype(jnp.float32)
    split_pieces = weight_matrix.reshape(N_TP, -1, weight_matrix.shape[1]).astype(jnp.float32)
    value_partial_sum = jnp.einsum('noc,oci->noi', block_list, split_pieces).astype(jnp.bfloat16)
    value_partial_sum = lax.optimization_barrier(value_partial_sum)
    return lax.optimization_barrier(jnp.sum(value_partial_sum.astype(jnp.float32), axis=1))

def channel_mixer(stream, gain, gate_weight, up_weight, down_weight):
    scaled, factor = norm_rows(stream, gain)
    gate = jnp.dot(scaled, gate_weight, preferred_element_type=jnp.float32) * factor
    up_sum = jnp.dot(scaled, up_weight, preferred_element_type=jnp.float32) * factor
    hidden = (jax.nn.silu(gate) * up_sum).astype(jnp.bfloat16)
    branch_output = blockwise_down(hidden, down_weight)
    return (stream.astype(jnp.float32) + 0.5 * branch_output).astype(jnp.bfloat16)

def token_mixer(stream, ssm_state, conv_state, gain, gate_in, value_in, write_in, read_in, step_in, conv_weight, step_bias, log_decay_rate, group_gain, out_weight):
    scaled, factor = norm_rows(stream, gain)

    def project(weight_matrix):
        return (jnp.dot(scaled, weight_matrix, preferred_element_type=jnp.float32) * factor).astype(jnp.bfloat16)
    gate = project(gate_in)
    values = project(value_in)
    writes = project(write_in)
    reads = project(read_in)
    steps = project(step_in)
    batch = stream.shape[0]
    groups = conv_weight.shape[1]
    state_size = write_in.shape[1] // groups
    heads = step_in.shape[1]
    head_size = value_in.shape[1] // heads
    per_group = heads // groups
    width = per_group * head_size
    fresh = jnp.concatenate([values.reshape(batch, groups, width), writes.reshape(batch, groups, state_size), reads.reshape(batch, groups, state_size)], axis=2)
    window = jnp.concatenate([conv_state, fresh[:, None]], axis=1)
    activated = jax.nn.silu(lax.optimization_barrier(jnp.sum(window.astype(jnp.float32) * conv_weight.astype(jnp.float32)[None], axis=1)))
    inputs = activated[:, :, :width].reshape(batch, groups, per_group, head_size)
    write_vec = activated[:, :, width:width + state_size]
    read_vec = activated[:, :, width + state_size:]
    step_size = jax.nn.softplus(steps.astype(jnp.float32) + step_bias[None])
    decay = jnp.exp(-step_size * jnp.exp(log_decay_rate)[None])
    step_size = step_size.reshape(batch, groups, per_group)
    decay = decay.reshape(batch, groups, per_group)
    carried = ssm_state.reshape(batch, groups, per_group, head_size, state_size)
    updated = carried * decay[:, :, :, None, None] + (step_size[:, :, :, None] * inputs)[..., None] * write_vec[:, :, None, None, :]
    readout = jnp.einsum('bghpn,bgn->bghp', updated, read_vec).reshape(batch, groups, width)
    gated = readout * jax.nn.silu(gate.astype(jnp.float32)).reshape(batch, groups, width)
    normed = gated * lax.rsqrt(lax.optimization_barrier(jnp.mean(gated * gated, axis=2, keepdims=True)) + norm_epsilon)
    mixed = (normed * group_gain.reshape(groups, width)[None]).astype(jnp.bfloat16).reshape(batch, groups * width)
    branch_output = blockwise_down(mixed, out_weight)
    after = (stream.astype(jnp.float32) + branch_output).astype(jnp.bfloat16)
    return (after, updated.reshape(ssm_state.shape), window[:, 1:])

def reference(stream, ssm_state, conv_state, first_gain, first_gate, first_up, first_down, mix_gain, gate_in, value_in, write_in, read_in, step_in, conv_weight, step_bias, log_decay_rate, group_gain, out_weight, last_norm_gain, second_gate, second_up, second_down):
    after_first = channel_mixer(stream, first_gain, first_gate, first_up, first_down)
    after_mix, ssm_next, conv_next = token_mixer(after_first, ssm_state, conv_state, mix_gain, gate_in, value_in, write_in, read_in, step_in, conv_weight, step_bias, log_decay_rate, group_gain, out_weight)
    next_stream = channel_mixer(after_mix, last_norm_gain, second_gate, second_up, second_down)
    return (next_stream, ssm_next, conv_next)
```

```python
import functools

import jax
import jax.numpy as jnp
from jax import lax
from jax.experimental import pallas as pl
from jax.experimental.pallas import tpu as pltpu
from jax.sharding import PartitionSpec as P

norm_epsilon = 1e-06
MESH = pl.DeviceIdType.MESH
LANES = 128
VM = pl.BlockSpec(memory_space=pltpu.VMEM)
HB = pl.BlockSpec(memory_space=pltpu.HBM)
F32 = jnp.float32
BF16 = jnp.bfloat16


def sigmoid_gate(v):
    return v / (1.0 + jnp.exp(-v))


def copy_to(src, dst, send, recv, **where):
    return pltpu.make_async_remote_copy(
        src_ref=src, dst_ref=dst, send_sem=send, recv_sem=recv, device_id=where, device_id_type=MESH
    )


class Plan:
    def __init__(self):
        self.names, self.shapes = [], []

    def add(self, name, shape, dtype):
        self.names.append(name)
        self.shapes.append(pltpu.VMEM(shape, dtype))

    def sem(self, name, *shape):
        self.names.append(name)
        self.shapes.append(pltpu.SemaphoreType.DMA(shape or (1,)))


def cut(total, shares):
    ends = [0] + [max(1, round(total * s)) for s in shares] + [total]
    return [(a, b) for a, b in zip(ends, ends[1:]) if b > a]


class Sizes:
    def __init__(self, n, nt, rows, depth, units, heads, head, state, groups, split):
        self.n, self.nt, self.rows, self.depth, self.units = n, nt, rows, depth, units
        self.heads, self.head, self.state, self.groups, self.split = heads, head, state, groups, split
        self.zn, self.zh, self.ny = n // 2, n // 4, nt // 2
        self.count, self.half = rows // n, rows // 2
        tiles = units // LANES
        b = max(1, tiles // 4)
        self.ff_a = cut(tiles - b, (0.2, 0.5, 0.8))
        self.ff_b = (tiles - b, tiles)
        self.inner = heads * head
        self.group_width = self.inner // groups
        self.channels = self.group_width + 2 * state
        v, g = self.inner // LANES, self.inner // LANES
        gb = max(1, g * 5 // 8)
        vec = groups * state
        self.mix_chunks = [
            [("value", 0, v // 2 * LANES)],
            [("value", v // 2 * LANES, v * LANES), ("write", 0, vec)],
            [("read", 0, vec), ("step", 0, LANES), ("gate", gb * LANES, g * LANES)],
            [("gate", 0, gb * LANES)],
        ]
        spans, at = [], 0
        self.place = {}
        for chunk in self.mix_chunks:
            lo = at
            for name, a, z in chunk:
                self.place[name, a] = (at, z - a)
                at += z - a
            spans.append((lo, at))
        self.mix_a, self.mix_b, self.mix_width = spans[:-1], spans[-1], at


def add_sum(plan, s, p, width, bwidth, achunks):
    zn, zh, cnt, n = s.zn, s.zh, s.count, s.n
    plan.add(p + "part", (zh, 2, 2, cnt, width), BF16)
    plan.add(p + "near", (zh, 2, cnt, width - bwidth), BF16)
    plan.add(p + "mid", (zh, 2, cnt, width - bwidth), BF16)
    plan.add(p + "far", (zn - 1, cnt, width - bwidth), BF16)
    plan.add(p + "b1", (zh, 2, cnt, bwidth), BF16)
    plan.add(p + "b2", (zh, 2, cnt, bwidth), BF16)
    plan.add(p + "b3", (zh, cnt, bwidth), BF16)
    plan.add(p + "b4", (zh, cnt, bwidth), BF16)
    plan.add(p + "b5", (max(1, zh - 1), cnt, bwidth), BF16)
    plan.add(p + "side", (n, cnt, LANES), F32)
    plan.add(p + "sides", (n - 1, cnt, LANES), F32)
    for k in "sr":
        plan.sem(p + "x" + k, achunks)
        plan.sem(p + "z" + k, achunks, zn - 1)
        plan.sem(p + "p" + k)
        plan.sem(p + "q" + k)
        plan.sem(p + "c" + k, max(1, zh - 1))
        plan.sem(p + "e" + k, n - 1)


def add_spread(plan, s, p, width, achunks, with_b):
    plan.add(p + "hid", (s.zh, 2, 2, s.count, width), BF16)
    for k in "sr":
        plan.sem(p + "h" + k, achunks, s.zn - 1)
        plan.sem(p + "g" + k, achunks)
        if with_b:
            plan.sem(p + "i" + k, max(1, s.zh - 1))
            plan.sem(p + "j" + k)
            plan.sem(p + "k" + k)


def add_finish(plan, s, p, last):
    plan.add(p + "acc", (s.rows, s.depth), F32)
    if last and not s.split:
        plan.add(p + "t0", (s.nt, s.rows, s.depth // s.nt), BF16)
        plan.add(p + "t1", (s.nt - 1, s.rows, s.depth // s.nt), BF16)
        for k in "sr":
            plan.sem(p + "t" + k, s.nt - 1)
        return
    plan.add(p + "t0", (2, s.half, s.depth), BF16)
    plan.add(p + "t1", (s.half, s.depth), BF16)
    plan.add(p + "t2", (s.half, s.depth), BF16)
    plan.add(p + "t3", (max(1, s.ny - 1), s.half, s.depth), BF16)
    plan.add(p + "feat", (2, s.half, s.depth), BF16)
    for k in "sr":
        plan.sem(p + "t" + k)
        plan.sem(p + "u" + k, max(1, s.ny - 1))
        plan.sem(p + "v" + k)


def make_plan(s, weights):
    plan = Plan()
    for name, shape, dtype in weights:
        plan.add("v_" + name, shape, dtype)
    plan.sem("w", len(weights))
    plan.sem("w1", 2, len(s.ff_a) + 1)
    plan.add("feat", (2, s.half, s.depth), BF16)
    plan.add("gains", (s.nt, 3, s.depth // s.nt) if not s.split else (1, 3, s.depth), F32)
    plan.sem("l0", 4)
    for k in "sr":
        plan.sem("f" + k, s.nt - 1)
        plan.sem("n" + k, s.nt - 1)
    fb = (s.ff_b[1] - s.ff_b[0]) * LANES
    for p in ("1", "2"):
        add_sum(plan, s, p, 2 * s.units, 2 * fb, len(s.ff_a))
        add_spread(plan, s, p, s.units, len(s.ff_a), True)
    add_sum(plan, s, "m", s.mix_width, s.mix_b[1] - s.mix_b[0], len(s.mix_a))
    add_spread(plan, s, "m", s.inner, s.groups, False)
    add_finish(plan, s, "1", False)
    add_finish(plan, s, "m", False)
    add_finish(plan, s, "2", True)
    plan.add("proj", (s.count, s.mix_width), F32)
    plan.add("conv", (s.groups, s.count, s.channels), F32)
    plan.add("vecs", (s.groups, s.count, s.state), BF16)
    return plan


class Body:
    def __init__(self, s, r):
        self.s, self.r, self.sent = s, r, []
        me = lax.axis_index("kv")
        self.me, self.z, self.x = me, me // 2, lax.rem(me, 2)
        self.q, self.par = me // 4, lax.rem(me // 2, 2)
        self.tp = lax.axis_index("tp")
        self.y, self.core = self.tp // 2, lax.rem(self.tp, 2)
        self.xpeer = self.z * 2 + 1 - self.x
        self.ppeer = (self.q * 2 + 1 - self.par) * 2 + self.x

    def start(self, copy):
        copy.start()
        self.sent.append(copy)
        return copy

    def send(self, src, dst, sem, *index, **where):
        s, r = self.r[sem + "s"], self.r[sem + "r"]
        index = index or (0,)
        return self.start(copy_to(src, dst, s.at[index], r.at[index], **where))

    def local(self, src, dst, sem):
        copy = pltpu.make_async_copy(src, dst, sem)
        copy.start()
        return copy

    def side_send(self, p):
        side, sides = self.r[p + "side"], self.r[p + "sides"]
        self.sides = []
        for d in range(1, self.s.n):
            k = lax.rem(self.me + d, self.s.n)
            self.sides.append(self.send(side.at[k], sides.at[d - 1], p + "e", d - 1, kv=k))

    def side_total(self, p):
        total = self.r[p + "side"][self.me]
        for d, copy in enumerate(self.sides):
            copy.wait_recv()
            total = total + self.r[p + "sides"][d]
        return total

    def x_send(self, p, c, lo, hi):
        cols = pl.ds(lo, hi - lo)
        r = self.r
        return self.send(
            r[p + "part"].at[:, :, 1 - self.x, :, cols], r[p + "near"].at[:, :, :, cols], p + "x", c, kv=self.xpeer
        )

    def z_send(self, p, c, lo, hi, copy):
        cols = pl.ds(lo, hi - lo)
        r, s = self.r, self.s
        copy.wait_recv()
        total = r[p + "part"][:, :, self.x, :, cols].astype(F32) + r[p + "near"][:, :, :, cols].astype(F32)
        r[p + "mid"][:, :, :, cols] = total.astype(BF16)
        copies = []
        for d in range(1, s.zn):
            zp = lax.rem(self.z + d, s.zn)
            copies.append(
                self.send(
                    r[p + "mid"].at[zp // 2, lax.rem(zp, 2), :, cols],
                    r[p + "far"].at[d - 1, :, cols],
                    p + "z", c, d - 1, kv=zp * 2 + self.x,
                )
            )
        return copies

    def z_total(self, p, lo, hi, copies):
        cols = pl.ds(lo, hi - lo)
        r = self.r
        total = r[p + "mid"][self.q, self.par, :, cols].astype(F32)
        for d, copy in enumerate(copies):
            copy.wait_recv()
            total = total + r[p + "far"][d, :, cols].astype(F32)
        return total

    def p_send(self, p, lo, hi):
        r = self.r
        cols = pl.ds(lo, hi - lo)
        return self.send(r[p + "part"].at[:, 1 - self.par, :, :, cols], r[p + "b1"], p + "p", kv=self.ppeer)

    def q_send(self, p, lo, hi, copy):
        r = self.r
        copy.wait_recv()
        total = r[p + "part"][:, self.par, :, :, pl.ds(lo, hi - lo)].astype(F32) + r[p + "b1"][...].astype(F32)
        r[p + "b2"][...] = total.astype(BF16)
        return self.send(r[p + "b2"].at[:, 1 - self.x], r[p + "b3"], p + "q", kv=self.xpeer)

    def c_send(self, p, copy):
        r, s = self.r, self.s
        copy.wait_recv()
        total = r[p + "b2"][:, self.x].astype(F32) + r[p + "b3"][...].astype(F32)
        r[p + "b4"][...] = total.astype(BF16)
        copies = []
        for d in range(1, s.zh):
            qp = lax.rem(self.q + d, s.zh)
            copies.append(
                self.send(
                    r[p + "b4"].at[qp], r[p + "b5"].at[d - 1], p + "c", d - 1, kv=(qp * 2 + self.par) * 2 + self.x
                )
            )
        return copies

    def c_total(self, p, copies):
        r = self.r
        total = r[p + "b4"][self.q].astype(F32)
        for d, copy in enumerate(copies):
            copy.wait_recv()
            total = total + r[p + "b5"][d].astype(F32)
        return total

    def spot(self, p, z, cols):
        return self.r[p + "hid"].at[z // 2, lax.rem(z, 2), self.x, :, cols]

    def h_send(self, p, c, cols):
        s = self.s
        mine = self.spot(p, self.z, cols)
        for d in range(1, s.zn):
            zp = lax.rem(self.z + d, s.zn)
            self.send(mine, mine, p + "h", c, d - 1, kv=zp * 2 + self.x)

    def arrived(self, place, sem, *index, **where):
        index = index or (0,)
        copy_to(place, place, self.r[sem + "s"].at[index], self.r[sem + "r"].at[index], **where).wait_recv()

    def g_send(self, p, c, cols):
        s = self.s
        for d in range(1, s.zn):
            left = lax.rem(self.z - d + s.zn, s.zn)
            self.arrived(self.spot(p, left, cols), p + "h", c, d - 1, kv=left * 2 + self.x)
        block = self.r[p + "hid"].at[:, :, self.x, :, cols]
        self.send(block, block, p + "g", c, kv=self.xpeer)

    def g_wait(self, p, c, cols):
        self.arrived(self.r[p + "hid"].at[:, :, 1 - self.x, :, cols], p + "g", c, kv=self.xpeer)

    def i_send(self, p, cols):
        s = self.s
        mine = self.spot(p, self.z, cols)
        for d in range(1, s.zh):
            qp = lax.rem(self.q + d, s.zh)
            self.send(mine, mine, p + "i", d - 1, kv=(qp * 2 + self.par) * 2 + self.x)

    def j_send(self, p, cols):
        s = self.s
        for d in range(1, s.zh):
            left = lax.rem(self.q - d + s.zh, s.zh) * 2 + self.par
            self.arrived(self.spot(p, left, cols), p + "i", d - 1, kv=left * 2 + self.x)
        block = self.r[p + "hid"].at[:, self.par, self.x, :, cols]
        self.send(block, block, p + "j", kv=self.xpeer)

    def k_send(self, p, cols):
        hid = self.r[p + "hid"]
        self.arrived(hid.at[:, self.par, 1 - self.x, :, cols], p + "j", kv=self.xpeer)
        block = hid.at[:, self.par, :, :, cols]
        self.send(block, block, p + "k", kv=self.ppeer)

    def k_wait(self, p, cols):
        self.arrived(self.r[p + "hid"].at[:, 1 - self.par, :, :, cols], p + "k", kv=self.ppeer)

    def finish(self, p, weight, before):
        r, s = self.r, self.s
        t0, t1, t2, t3, feat = (r[p + k] for k in ("t0", "t1", "t2", "t3", "feat"))
        t0[...] = r[p + "acc"][...].astype(BF16).reshape(2, s.half, s.depth)
        other = self.tp + 1 - 2 * self.core
        copy = self.send(t0.at[1 - self.core], t1, p + "t", tp=other)
        copy.wait_recv()
        t2[...] = (t0[self.core].astype(F32) + t1[...].astype(F32)).astype(BF16)
        copies = []
        for d in range(1, s.ny):
            yp = lax.rem(self.y + d, s.ny)
            copies.append(self.send(t2, t3.at[d - 1], p + "u", d - 1, tp=yp * 2 + self.core))
        total = t2[...].astype(F32)
        for d, copy in enumerate(copies):
            copy.wait_recv()
            total = total + t3[d].astype(F32)
        feat[self.core] = (before[self.core].astype(F32) + weight * total).astype(BF16)
        mine = feat.at[self.core]
        self.send(mine, mine, p + "v", tp=other)
        self.arrived(feat.at[1 - self.core], p + "v", tp=other)
        return feat

    def finish_last(self, p, weight, before, out_ref):
        r, s = self.r, self.s
        if s.split:
            feat = Body.finish_split(self, p, weight, before)
            out_ref[...] = feat[...].reshape(s.rows, s.depth)
            return
        width = s.depth // s.nt
        t0, t1 = r[p + "t0"], r[p + "t1"]
        for k in range(s.nt):
            t0[k] = r[p + "acc"][:, k * width : (k + 1) * width].astype(BF16)
        copies = []
        for d in range(1, s.nt):
            k = lax.rem(self.tp + d, s.nt)
            copies.append(self.send(t0.at[k], t1.at[d - 1], p + "t", d - 1, tp=k))
        total = t0[self.tp].astype(F32)
        for d, copy in enumerate(copies):
            copy.wait_recv()
            total = total + t1[d].astype(F32)
        cols = pl.ds(pl.multiple_of(self.tp * width, LANES), width)
        mine = before[:, :, cols].astype(F32).reshape(s.rows, width)
        out_ref[...] = (mine + weight * total).astype(BF16)

    def finish_split(self, p, weight, before):
        return self.finish(p, weight, before)

    def gain(self, k):
        gains = self.r["gains"]
        return jnp.concatenate([gains[t, k : k + 1, :] for t in range(gains.shape[0])], axis=1)

    def normed(self, p, feat, k):
        s = self.s
        values = feat[...].reshape(s.rows, s.depth).astype(F32)
        squares = jnp.sum(values * values, axis=1, keepdims=True)
        self.r[p + "side"][...] = jnp.broadcast_to(squares, (s.rows, LANES)).reshape(s.n, s.count, LANES)
        return (values * self.gain(k)).astype(BF16)

    def put_part(self, p, lo, value):
        s = self.s
        w = value.shape[1]
        self.r[p + "part"][:, :, :, :, pl.ds(lo, w)] = value.astype(BF16).reshape(s.zh, 2, 2, s.count, w)

    def feed_forward(self, p, feat, k, ready):
        s, r = self.s, self.r
        gate, up, down = (r["v_" + w + p] for w in ("gate", "up", "down"))
        acc = r[p + "acc"]
        scaled = self.normed(p, feat, k)
        spans = s.ff_a + [s.ff_b]
        b = len(s.ff_a)

        def span(c, scale=1):
            return spans[c][0] * LANES * scale, spans[c][1] * LANES * scale

        def cols(c):
            lo, hi = span(c)
            return pl.ds(lo, hi - lo)

        def multiply(c):
            ready(c)
            lo, hi = span(c)
            for i, w in enumerate((gate, up)):
                value = jnp.dot(scaled, w[:, lo:hi], preferred_element_type=F32)
                self.put_part(p, 2 * lo + i * (hi - lo), value)

        def activate(c, total):
            lo, hi = span(c)
            total = total * self.factor
            hidden = sigmoid_gate(total[:, : hi - lo]) * total[:, hi - lo :]
            r[p + "hid"][self.q, self.par, self.x, :, pl.ds(lo, hi - lo)] = hidden.astype(BF16)

        def lower(c):
            lo, hi = span(c)
            if c < b:
                self.g_wait(p, c, cols(c))
            else:
                self.k_wait(p, cols(c))
            hidden = r[p + "hid"][:, :, :, :, pl.ds(lo, hi - lo)].reshape(s.rows, hi - lo)
            value = jnp.dot(hidden, down[lo:hi, :], preferred_element_type=F32)
            if c == 0:
                acc[...] = value
            else:
                acc[...] += value

        xs, zs = {}, {}
        many = range(b)

        def start(c):
            multiply(c)
            xs[c] = self.x_send(p, c, *span(c, 2))

        def along(c):
            zs[c] = self.z_send(p, c, *span(c, 2), xs[c])

        def spread(c):
            activate(c, self.z_total(p, *span(c, 2), zs[c]))
            self.h_send(p, c, cols(c))

        def forward(c):
            self.g_send(p, c, cols(c))

        start(0)
        multiply(b)
        pair = self.p_send(p, *span(b, 2))
        self.side_send(p)
        for c in many[1:-1]:
            start(c)
        along(0)
        self.factor = None
        second = self.q_send(p, *span(b, 2), pair)
        start(b - 1)
        squares = self.side_total(p)
        self.factor = lax.rsqrt(squares / (s.depth * s.n) + norm_epsilon)[:, :1]
        along(1)
        spread(0)
        along(2)
        cross = self.c_send(p, second)
        spread(1)
        for c in many[3:]:
            along(c)
        forward(0)
        activate(b, self.c_total(p, cross))
        self.i_send(p, cols(b))
        spread(2)
        forward(1)
        for c in many[3:]:
            spread(c)
        self.j_send(p, cols(b))
        forward(2)
        lower(0)
        self.k_send(p, cols(b))
        for c in many[3:]:
            forward(c)
        lower(1)
        lower(2)
        lower(b)
        for c in many[3:]:
            lower(c)

    def mixer(self, p, feat, outs):
        s, r = self.s, self.r
        fresh_ref, si_ref, decay_ref, write_ref = outs
        scaled = self.normed(p, feat, 1)
        side = r[p + "side"]
        spans = s.mix_a + [s.mix_b]
        b = len(s.mix_a)
        proj = r["proj"]

        def multiply(c):
            for name, lo, hi in s.mix_chunks[c]:
                at, w = s.place[name, lo]
                weight = r["v_" + name]
                if name == "step":
                    value = jnp.dot(scaled, weight[...], preferred_element_type=F32)
                    self.put_part(p, at, jnp.zeros((s.rows, LANES), F32))
                    self.put_part(p, at, value)
                else:
                    self.put_part(p, at, jnp.dot(scaled, weight[:, lo:hi], preferred_element_type=F32))

        def keep(c, total):
            lo, hi = spans[c]
            proj[:, lo:hi] = (total * self.factor).astype(BF16).astype(F32)

        xs, zs = {}, {}
        multiply(0)
        xs[0] = self.x_send(p, 0, *spans[0])
        multiply(b)
        pair = self.p_send(p, *spans[b])
        self.side_send(p)
        multiply(1)
        xs[1] = self.x_send(p, 1, *spans[1])
        multiply(2)
        self.conv_past()
        zs[0] = self.z_send(p, 0, *spans[0], xs[0])
        second = self.q_send(p, *spans[b], pair)
        xs[2] = self.x_send(p, 2, *spans[2])
        zs[1] = self.z_send(p, 1, *spans[1], xs[1])
        cross = self.c_send(p, second)
        squares = self.side_total(p)
        self.factor = lax.rsqrt(squares / (s.depth * s.n) + norm_epsilon)[:, :1]
        keep(0, self.z_total(p, *spans[0], zs[0]))
        zs[2] = self.z_send(p, 2, *spans[2], xs[2])
        keep(1, self.z_total(p, *spans[1], zs[1]))
        keep(b, self.c_total(p, cross))
        keep(2, self.z_total(p, *spans[2], zs[2]))

        def take(name):
            pieces = []
            for chunk in s.mix_chunks:
                for other, lo, _ in chunk:
                    if other == name:
                        pieces.append((lo, *s.place[name, lo]))
            return jnp.concatenate([proj[:, at : at + w] for _, at, w in sorted(pieces)], axis=1)

        values, writes, reads = take("value"), take("write"), take("read")
        at, _ = s.place["step", 0]
        steps = proj[:, at : at + LANES][:, : s.heads]
        step = jax.nn.softplus(steps + r["v_bias"][...])
        decay = jnp.exp(-step * jnp.exp(r["v_rate"][...]))
        head_row = lax.broadcasted_iota(jnp.int32, (s.heads, s.inner), 0)
        head_col = lax.broadcasted_iota(jnp.int32, (s.heads, s.inner), 1) // s.head
        widen = (head_row == head_col).astype(F32)
        exact = dict(preferred_element_type=F32, precision=lax.Precision.HIGHEST)
        step_wide = jnp.dot(step, widen, **exact)
        decay_wide = jnp.dot(decay, widen, **exact)
        decay_ref[...] = decay_wide
        gw, st = s.group_width, s.state
        conv_w = r["v_conv_w"]
        taps = conv_w.shape[0]
        gates = take("gate")
        scaled_inputs, lone, activated = [], [], []
        for g in range(s.groups):
            fresh = jnp.concatenate(
                [values[:, g * gw : (g + 1) * gw], writes[:, g * st : (g + 1) * st], reads[:, g * st : (g + 1) * st]],
                axis=1,
            )
            fresh_ref[g] = fresh
            act = sigmoid_gate(r["conv"][g] + fresh * conv_w[taps - 1, g : g + 1, :])
            inputs, write, read = act[:, :gw], act[:, gw : gw + st], act[:, gw + st :]
            si = inputs * step_wide[:, g * gw : (g + 1) * gw]
            si_ref[:, g * gw : (g + 1) * gw] = si
            write_ref[:, g * st : (g + 1) * st] = write
            r["vecs"][g] = read.astype(BF16)
            scaled_inputs.append(si)
            lone.append(jnp.sum(write * read, axis=1, keepdims=True))
        state = r["v_state"]
        per = s.heads // s.groups
        row = lax.broadcasted_iota(jnp.int32, (s.count, s.state), 0)
        for g in range(s.groups):

            def one(k, total, g=g):
                held = state[k, g * per : (g + 1) * per].reshape(gw, st).astype(BF16)
                vec = r["vecs"][g]
                vec = jnp.where(row == k, vec.astype(F32), 0.0).astype(BF16)
                return total + lax.dot_general(
                    vec, held, (((1,), (1,)), ((), ())), preferred_element_type=F32
                )

            drawn = lax.fori_loop(0, s.count, one, jnp.zeros((s.count, gw), F32))
            cols = slice(g * gw, (g + 1) * gw)
            readout = decay_wide[:, cols] * drawn + scaled_inputs[g] * lone[g]
            gated = readout * sigmoid_gate(gates[:, cols])
            mean = jnp.sum(gated * gated, axis=1, keepdims=True) / gw
            mixed = gated * lax.rsqrt(mean + norm_epsilon) * r["v_group_gain"][:, cols]
            r[p + "hid"][self.q, self.par, self.x, :, pl.ds(g * gw, gw)] = mixed.astype(BF16)
            self.h_send(p, g, pl.ds(g * gw, gw))
        for g in range(s.groups):
            self.g_send(p, g, pl.ds(g * gw, gw))
        acc = r[p + "acc"]
        for g in range(s.groups):
            cols = pl.ds(g * gw, gw)
            self.g_wait(p, g, cols)
            mixed = r[p + "hid"][:, :, :, :, cols].reshape(s.rows, gw)
            value = jnp.dot(mixed, r["v_out"][g * gw : (g + 1) * gw, :], preferred_element_type=F32)
            if g == 0:
                acc[...] = value
            else:
                acc[...] += value

    def conv_past(self):
        s, r = self.s, self.r
        past, weight, conv = r["v_conv_state"], r["v_conv_w"], r["conv"]
        taps = weight.shape[0]

        def one(k, carry):
            total = past[k, 0].astype(F32) * weight[0]
            for t in range(1, taps - 1):
                total = total + past[k, t].astype(F32) * weight[t]
            for g in range(s.groups):
                conv[g, pl.ds(k, 1), :] = total[g : g + 1, :]
            return carry

        lax.fori_loop(0, s.count, one, 0)


def step_kernel(s, plan, names, *refs):
    count = len(names)
    hbm = dict(zip(names, refs[:count]))
    outs = refs[count : count + 5]
    r = dict(zip(plan.names, refs[count + 5 :]))
    body = Body(s, r)
    order = [n for n in names if n not in ("stream", "gain1", "gain2", "gain3")]
    gains = r["gains"]
    width = s.depth // s.nt
    spans = s.ff_a + [s.ff_b]
    head = []
    if s.split:
        head.append(body.local(hbm["stream"], r["feat"], r["l0"].at[0]))
        head.append(body.local(hbm["gain1"], gains.at[0], r["l0"].at[1]))
    else:
        mine = pl.ds(pl.multiple_of(body.tp * width, LANES), width)
        head.append(body.local(hbm["stream"], r["feat"].at[:, :, mine], r["l0"].at[0]))
        for k in range(3):
            head.append(body.local(hbm["gain%d" % (k + 1)], gains.at[body.tp, pl.ds(k, 1)], r["l0"].at[k + 1]))
    first = {}
    for c in [0, len(spans) - 1] + list(range(1, len(spans) - 1)):
        lo, hi = spans[c]
        cols = pl.ds(lo * LANES, (hi - lo) * LANES)
        for i, name in enumerate(("gate1", "up1")):
            first[c, i] = body.local(hbm[name].at[:, cols], r["v_" + name].at[:, cols], r["w1"].at[i, c])
    sem = pltpu.get_barrier_semaphore()
    for d in range(1, s.n):
        pl.semaphore_signal(sem, inc=1, device_id={"kv": lax.rem(body.me + d, s.n)}, device_id_type=MESH)
    for d in range(1, s.nt):
        pl.semaphore_signal(sem, inc=1, device_id={"tp": lax.rem(body.tp + d, s.nt)}, device_id_type=MESH)
    pl.semaphore_wait(sem, s.n + s.nt - 2)
    for copy in head:
        copy.wait()
    if not s.split:
        block = r["feat"].at[:, :, mine]
        for d in range(1, s.nt):
            k = lax.rem(body.tp + d, s.nt)
            body.send(block, block, "f", d - 1, tp=k)
            body.send(gains.at[body.tp], gains.at[body.tp], "n", d - 1, tp=k)
        for d in range(1, s.nt):
            left = lax.rem(body.tp - d + s.nt, s.nt)
            place = r["feat"].at[:, :, pl.ds(pl.multiple_of(left * width, LANES), width)]
            body.arrived(place, "f", d - 1, tp=left)
            body.arrived(gains.at[left], "n", d - 1, tp=left)
    rest = {}

    def ready(c):
        first[c, 0].wait()
        first[c, 1].wait()
        if c == 0:
            for i, name in enumerate(order):
                if name not in ("gate1", "up1"):
                    rest[name] = body.local(hbm[name], r["v_" + name], r["w"].at[i])

    waited = set()

    def need(*wanted):
        for name in wanted:
            if name not in waited:
                waited.add(name)
                rest[name].wait()

    plain_lower = body.g_wait

    def g_wait(p, c, cols):
        plain_lower(p, c, cols)
        need({"1": "down1", "2": "down2", "m": "out"}[p])

    body.g_wait = g_wait
    body.feed_forward("1", r["feat"], 0, ready)
    after = body.finish("1", 0.5, r["feat"])
    need("value", "write", "read", "step", "gate", "bias", "rate", "conv_w", "group_gain", "conv_state", "state")
    body.mixer("m", after, outs[1:])
    after = body.finish("m", 1.0, after)
    need("gate2", "up2")
    body.feed_forward("2", after, 2, lambda c: None)
    body.finish_last("2", 0.5, after, outs[0])
    for copy in body.sent:
        copy.wait_send()


def update_kernel(s, block, state_ref, past_ref, fresh_ref, si_ref, decay_ref, write_ref, next_ref, *rest):
    state_out, past_out, next_out, left_ref = rest
    cnt, gw, st = s.count, s.group_width, s.state

    @pl.when(pl.program_id(0) == 0)
    def prepare():
        next_out[...] = next_ref[...]
        for g in range(s.groups):
            cols = slice(g * gw, (g + 1) * gw)
            si, decay = si_ref[:, cols], decay_ref[:, cols]
            high = si.astype(BF16).astype(F32)
            low = si - high
            d1 = decay.astype(BF16).astype(F32)
            d2 = (decay - d1).astype(BF16).astype(F32)
            d3 = decay - d1 - d2
            parts = [high, high, low, d1, d2, d3]
            parts.append(jnp.zeros((left_ref.shape[2] - len(parts) * cnt, gw), F32))
            left_ref[g] = jnp.concatenate(parts, axis=0).T.astype(BF16)

    row = lax.broadcasted_iota(jnp.int32, (cnt, st), 0)

    def one(i, carry):
        k = pl.program_id(0) * block + i
        here = row == k
        pick = jnp.where(here, 1.0, 0.0)
        zero = jnp.zeros((cnt, st), F32)
        per = s.heads // s.groups
        taps = past_ref.shape[1]
        newest = []
        for g in range(s.groups):
            write = jnp.where(here, write_ref[:, g * st : (g + 1) * st], 0.0)
            high = write.astype(BF16).astype(F32)
            low = write - high
            side = jnp.concatenate([high, low, high, zero, zero, zero], axis=0)
            ones = jnp.concatenate([zero, zero, zero, pick, pick, pick], axis=0)
            right = jnp.concatenate([side, ones], axis=1)
            fill = left_ref.shape[2] - right.shape[0]
            right = jnp.concatenate([right, jnp.zeros((fill, 2 * st), F32)], axis=0).astype(BF16)
            both = jnp.dot(left_ref[g], right, preferred_element_type=F32)
            held = state_ref[i, g * per : (g + 1) * per].reshape(gw, st)
            state_out[i, g * per : (g + 1) * per] = (held * both[:, st:] + both[:, :st]).reshape(per, s.head, st)
            newest.append(fresh_ref[g, pl.ds(k, 1), :])
        for t in range(taps - 1):
            past_out[i, t] = past_ref[i, t + 1]
        past_out[i, taps - 1] = jnp.concatenate(newest, axis=0).astype(BF16)
        return carry

    lax.fori_loop(0, block, one, 0)


def gathered(stream, gains):
    n = lax.axis_size("tp")
    features = lax.all_gather(stream, "tp", axis=1, tiled=True)
    packed = lax.all_gather(jnp.stack(gains), "tp", axis=1, tiled=True)
    return features, packed


def on_device(
    stream,
    ssm_state,
    conv_state,
    first_gain,
    first_gate,
    first_up,
    first_down,
    mix_gain,
    gate_in,
    value_in,
    write_in,
    read_in,
    step_in,
    conv_weight,
    step_bias,
    log_decay_rate,
    group_gain,
    out_weight,
    last_norm_gain,
    second_gate,
    second_up,
    second_down,
):
    n, nt = lax.axis_size("kv"), lax.axis_size("tp")
    rows, width = stream.shape
    depth, units = first_gate.shape
    heads, head, state = ssm_state.shape[1:]
    groups = conv_weight.shape[1]
    split = width % LANES != 0
    s = Sizes(n, nt, rows, depth, units, heads, head, state, groups, split)
    if split:
        features, packed = gathered(stream, [first_gain, mix_gain, last_norm_gain])
        named = {"stream": features.reshape(2, s.half, depth), "gain1": packed}
    else:
        named = {
            "stream": stream.reshape(2, s.half, width),
            "gain1": first_gain[None],
            "gain2": mix_gain[None],
            "gain3": last_norm_gain[None],
        }
    weights = {
        "gate1": first_gate,
        "up1": first_up,
        "down1": first_down,
        "value": value_in,
        "gate": gate_in,
        "write": write_in,
        "read": read_in,
        "step": step_in,
        "conv_w": conv_weight,
        "bias": step_bias[None],
        "rate": log_decay_rate[None],
        "group_gain": group_gain[None],
        "conv_state": conv_state,
        "state": ssm_state,
        "out": out_weight,
        "gate2": second_gate,
        "up2": second_up,
        "down2": second_down,
    }
    plan = make_plan(s, [(k, v.shape, v.dtype) for k, v in weights.items()])
    named.update(weights)
    cnt = s.count
    out_width = depth if split else width
    outs = [
        jax.ShapeDtypeStruct((rows, out_width), BF16),
        jax.ShapeDtypeStruct((groups, cnt, s.channels), F32),
        jax.ShapeDtypeStruct((cnt, s.inner), F32),
        jax.ShapeDtypeStruct((cnt, s.inner), F32),
        jax.ShapeDtypeStruct((cnt, groups * state), F32),
    ]
    result, fresh, si, decay, write = pl.pallas_call(
        functools.partial(step_kernel, s, plan, list(named)),
        out_shape=outs,
        in_specs=[HB] * len(named),
        out_specs=[VM] * len(outs),
        scratch_shapes=plan.shapes,
        compiler_params=pltpu.CompilerParams(
            collective_id=0, has_side_effects=True, vmem_limit_bytes=56 * 1024 * 1024
        ),
    )(*named.values())
    if split:
        me = lax.axis_index("tp")
        result = lax.dynamic_slice_in_dim(result, me * width, width, axis=1)
    block = 2
    deep = -(-6 * cnt // LANES) * LANES

    def rows_of(*dims):
        return pl.BlockSpec((block,) + dims, lambda i: (i,) + (0,) * len(dims))

    def whole(array):
        return pl.BlockSpec(array.shape, lambda i: (0,) * array.ndim)

    state_next, past_next, stream_next = pl.pallas_call(
        functools.partial(update_kernel, s, block),
        grid=(cnt // block,),
        out_shape=[
            jax.ShapeDtypeStruct(ssm_state.shape, ssm_state.dtype),
            jax.ShapeDtypeStruct(conv_state.shape, conv_state.dtype),
            jax.ShapeDtypeStruct(stream.shape, BF16),
        ],
        in_specs=[rows_of(*ssm_state.shape[1:]), rows_of(*conv_state.shape[1:])]
        + [whole(a) for a in (fresh, si, decay, write, result)],
        out_specs=[rows_of(*ssm_state.shape[1:]), rows_of(*conv_state.shape[1:]), whole(stream)],
        scratch_shapes=[pltpu.VMEM((groups, s.group_width, deep), BF16)],
        compiler_params=pltpu.CompilerParams(vmem_limit_bytes=60 * 1024 * 1024),
    )(ssm_state, conv_state, fresh, si, decay, write, result)
    return (stream_next, state_next, past_next)


def solution(mesh):
    return jax.shard_map(
        on_device,
        mesh=mesh,
        in_specs=(
            P(None, ("kv", "tp")),
            P("kv", "tp", None, None),
            P("kv", None, "tp", None),
            P(("kv", "tp")),
            P("kv", "tp"),
            P("kv", "tp"),
            P("tp", "kv"),
            P(("kv", "tp")),
            P("kv", "tp"),
            P("kv", "tp"),
            P("kv", "tp"),
            P("kv", "tp"),
            P("kv", "tp"),
            P(None, "tp", None),
            P("tp"),
            P("tp"),
            P("tp"),
            P("tp", "kv"),
            P(("kv", "tp")),
            P("kv", "tp"),
            P("kv", "tp"),
            P("tp", "kv"),
        ),
        out_specs=(P(None, ("kv", "tp")), P("kv", "tp", None, None), P("kv", None, "tp", None)),
        check_vma=False,
    )
```

```python
import functools

import jax
import jax.numpy as jnp
from jax import lax
from jax.experimental import pallas as pl
from jax.experimental.pallas import tpu as pltpu
from jax.sharding import PartitionSpec as P

norm_epsilon = 1e-06
MESH = pl.DeviceIdType.MESH
LANES = 128
KV, TP = "kv", "tp"
DIRECT, THREE, FIRST = "d", "t", "f"
VM = pl.BlockSpec(memory_space=pltpu.VMEM)
HB = pl.BlockSpec(memory_space=pltpu.HBM)
F32 = jnp.float32
BF16 = jnp.bfloat16


def sigmoid_gate(v):
    return v / (1.0 + jnp.exp(-v))


def copy_to(src, dst, send, recv, **where):
    return pltpu.make_async_remote_copy(
        src_ref=src, dst_ref=dst, send_sem=send, recv_sem=recv, device_id=where, device_id_type=MESH
    )


def tag(p, stage, c):
    return p + stage + str(c)


class Plan:
    def __init__(self):
        self.names, self.shapes = [], []

    def add(self, name, shape, dtype):
        self.names.append(name)
        self.shapes.append(pltpu.VMEM(shape, dtype))

    def sem(self, name, *shape):
        self.names.append(name)
        self.shapes.append(pltpu.SemaphoreType.DMA(shape or (1,)))


def cut(total, shares):
    ends = [0] + [max(1, round(total * s)) for s in shares] + [total]
    return [(a, b) for a, b in zip(ends, ends[1:]) if b > a]


SUM = {DIRECT: "xz", THREE: "xpc", FIRST: "pxc"}
SPREAD = {DIRECT: "hg", THREE: "ijg", FIRST: "ijk"}
FF_CHUNKS = [(DIRECT, THREE, 4), (FIRST, FIRST, 6), (THREE, THREE, 7), (THREE, DIRECT, 5)]
MIX_WAYS = (DIRECT, FIRST, DIRECT, DIRECT)
PARTS, UPDATE, UPDATES = 2, 8, 4
ORDER = [
    10010, 10, 0, 20, 30, 1, 11, 10000, 21, 2, 31, 10020, 10030, 12,
    10011, 22, 10001, 13, 32, 3, 10021, 23, 10031, 10012, 10002, 4, 33, 10022,
    14, 24, 10032, 10003, 5, 15, 34, 10013, 25, 10023, 10033, 10004, 10014, 35,
    16, 10024, 26, 1000, 1001, 10034, 10005, 10015, 10025, 1002, 10035, 10016, 1003, 2000,
    10026, 11000, 2010, 2020, 2030, 11001, 2001, 2011, 2021, 11002, 2031, 11003, 12020, 12000,
    12010, 2012, 2032, 2022, 12001, 12021, 12030, 2002, 12011, 2013, 3000, 12031, 8010, 8030,
    8020, 12012, 4001, 4011, 12022, 12032, 12002, 8000, 12013, 13000, 4002, 4012, 5000, 5001,
    18000, 18020, 18030, 14001, 14011, 5002, 18010, 5003, 6000, 6020, 6010, 14012, 14002, 15000,
    6030, 15001, 6001, 15002, 6011, 6021, 15003, 16010, 16000, 6002, 16020, 6012, 6031, 16030,
    6022, 16011, 16001, 6032, 6003, 6013, 16021, 6023, 16031, 16002, 16012, 6033, 6004, 16022,
    6014, 16032, 6024, 16003, 6005, 6015, 16013, 6034, 16023, 6025, 16004, 16033, 6016, 16014,
    16024, 6035, 6026, 16034, 7000, 16015, 16025, 16005, 16016, 16035, 16026, 17000, 7001, 17001,
]


class Sizes:
    def __init__(self, n, nt, rows, depth, units, heads, head, state, groups, split):
        self.n, self.nt, self.rows, self.depth, self.units = n, nt, rows, depth, units
        self.heads, self.head, self.state, self.groups, self.split = heads, head, state, groups, split
        self.zn, self.zh, self.ny = n // 2, n // 4, nt // 2
        self.parts = PARTS
        self.all_rows, self.rows = rows, rows // PARTS
        self.count, self.half = self.rows // n, self.rows // 2
        self.deep = -(-3 * self.count // LANES) * LANES
        tiles = units // LANES
        shares = [share for _, _, share in FF_CHUNKS]
        ends = [sum(shares[: i + 1]) / sum(shares) for i in range(len(shares) - 1)]
        self.ff_chunks = [
            (out, back, a * LANES, z * LANES) for (out, back, _), (a, z) in zip(FF_CHUNKS, cut(tiles, ends))
        ]
        self.inner = heads * head
        self.group_width = self.inner // groups
        self.channels = self.group_width + 2 * state
        v = self.inner // LANES
        vec = groups * state
        gb = max(1, v * 5 // 8)
        self.mix_chunks = [
            [("value", 0, v // 2 * LANES)],
            [("gate", 0, gb * LANES)],
            [("value", v // 2 * LANES, v * LANES), ("write", 0, vec)],
            [("read", 0, vec), ("step", 0, LANES), ("gate", gb * LANES, v * LANES)],
        ]
        spans, at = [], 0
        self.place = {}
        for chunk in self.mix_chunks:
            lo = at
            for name, a, z in chunk:
                self.place[name, a] = (at, z - a)
                at += z - a
            spans.append((lo, at))
        self.mix_spans = [(way, None, a, z) for way, (a, z) in zip(MIX_WAYS, spans)]
        self.mix_width = at


def add_sum(plan, s, p, width, chunks):
    zn, zh, cnt, n = s.zn, s.zh, s.count, s.n
    zl = max(1, zh - 1)
    plan.add(p + "part", (zh, 2, 2, cnt, width), BF16)
    plan.add(p + "near", (zh, 2, cnt, width), BF16)
    plan.add(p + "mid", (zh, 2, cnt, width), BF16)
    plan.add(p + "far", (zn - 1, cnt, width), BF16)
    plan.add(p + "near2", (zh, cnt, width), BF16)
    plan.add(p + "mid2", (zh, cnt, width), BF16)
    plan.add(p + "far2", (zl, cnt, width), BF16)
    plan.add(p + "side", (n, s.count, LANES), F32)
    plan.add(p + "sides", (n - 1, s.count, LANES), F32)
    plan.sem(p + "e")
    for c, chunk in enumerate(chunks):
        for stage in SUM[chunk[0]]:
            plan.sem(p + stage + str(c))


def add_spread(plan, s, p, width, chunks):
    plan.add(p + "hid", (s.zh, 2, 2, s.count, width), BF16)
    for c, chunk in enumerate(chunks):
        for stage in SPREAD[chunk[1]]:
            plan.sem(p + stage + str(c))


def add_finish(plan, s, p, last):
    plan.add(p + "acc", (s.rows, s.depth), F32)
    if last and not s.split:
        plan.add(p + "t0", (s.nt, s.rows, s.depth // s.nt), BF16)
        plan.add(p + "t1", (s.nt - 1, s.rows, s.depth // s.nt), BF16)
        plan.sem(p + "t")
        return
    plan.add(p + "t0", (2, s.half, s.depth), BF16)
    plan.add(p + "t1", (s.half, s.depth), BF16)
    plan.add(p + "t2", (s.half, s.depth), BF16)
    plan.add(p + "t3", (max(1, s.ny - 1), s.half, s.depth), BF16)
    plan.add(p + "feat", (2, s.half, s.depth), BF16)
    for stage in "tuv":
        plan.sem(p + stage)


def make_plan(s, weights):
    plan = Plan()
    for name, shape, dtype in weights:
        if name != "state":
            plan.add("v_" + name, shape, dtype)
    plan.sem("w", len(weights))
    plan.sem("w1", 2, len(s.ff_chunks))
    plan.add("feat", (s.n, s.parts, s.count, s.depth), BF16)
    plan.add("gains", (s.nt, 3, s.depth // s.nt) if not s.split else (1, 3, s.depth), F32)
    plan.sem("l0", 4)
    plan.sem("sent")
    plan.sem("f")
    plan.sem("n")
    for part in range(s.parts):
        q = str(part)
        plan.add("b" + q, (2, s.half, s.depth), BF16)
        for p in ("1" + q, "2" + q):
            add_sum(plan, s, p, 2 * s.units, s.ff_chunks)
            add_spread(plan, s, p, s.units, s.ff_chunks)
        add_sum(plan, s, "m" + q, s.mix_width, s.mix_spans)
        add_spread(plan, s, "m" + q, s.inner, [(DIRECT, DIRECT)] * s.groups)
        add_finish(plan, s, "1" + q, False)
        add_finish(plan, s, "m" + q, False)
        add_finish(plan, s, "2" + q, True)
        plan.add("proj" + q, (s.count, s.mix_width), F32)
        plan.add("conv" + q, (s.groups, s.count, s.channels), F32)
        plan.add("vecs" + q, (s.groups, s.count, s.state), F32)
        plan.add("left" + q, (s.groups, s.group_width, s.deep), BF16)
        plan.add("write" + q, (s.groups, s.count, s.state), F32)
        plan.add("decay" + q, (s.count, s.heads), F32)
    return plan


def scoped(f):
    @functools.wraps(f)
    def inner(*args):
        tag = "_".join(str(a) for a in args if isinstance(a, (str, int)))
        with jax.named_scope(f.__name__ + "_" + tag):
            return f(*args)

    return inner


class Body:
    def __init__(self, s, r, part, sent):
        self.s, self.r, self.sent, self.part, self.tail = s, r, sent, part, str(part)
        self.stage = None
        me = lax.axis_index(KV)
        self.me, self.z, self.x = me, me // 2, lax.rem(me, 2)
        self.q, self.par = me // 4, lax.rem(me // 2, 2)
        self.tp = lax.axis_index(TP)
        self.y, self.core = self.tp // 2, lax.rem(self.tp, 2)
        self.xpeer = self.z * 2 + 1 - self.x
        self.ppeer = (self.q * 2 + 1 - self.par) * 2 + self.x

    def start(self, copy):
        copy.start()
        self.sent.append(copy)
        return copy

    def send(self, src, dst, sem, **where):
        return self.start(copy_to(src, dst, self.r["sent"].at[0], self.r[sem].at[0], **where))

    def came(self, place, sem):
        pltpu.make_async_copy(place, place, self.r[sem].at[0]).wait()

    def local(self, src, dst, sem):
        copy = pltpu.make_async_copy(src, dst, sem)
        copy.start()
        return copy

    @scoped
    def side_send(self, p):
        side, sides = self.r[p + "side"], self.r[p + "sides"]
        for d in range(1, self.s.n):
            k = lax.rem(self.me + d, self.s.n)
            self.send(side.at[k], sides.at[d - 1], p + "e", kv=k)

    @scoped
    def row_factor(self, p):
        s = self.s
        total = self.r[p + "side"][self.me]
        self.came(self.r[p + "sides"], p + "e")
        for d in range(s.n - 1):
            total = total + self.r[p + "sides"][d]
        return lax.rsqrt(total / (s.depth * s.n) + norm_epsilon)[:, :1]

    def columns(self, chunk, scale=1):
        return pl.ds(chunk[2] * scale, (chunk[3] - chunk[2]) * scale)

    def across(self, q):
        return (q * 2 + self.par) * 2 + self.x

    def sum_start(self, p, c, kind, cols):
        part, near = self.r[p + "part"], self.r[p + "near"].at[:, :, :, cols]
        if kind == FIRST:
            self.send(part.at[:, 1 - self.par, :, :, cols], near, tag(p, "p", c), kv=self.ppeer)
        else:
            self.send(part.at[:, :, 1 - self.x, :, cols], near, tag(p, "x", c), kv=self.xpeer)

    @scoped
    def sum_step(self, p, name, c, kind, cols):
        r, s = self.r, self.s
        part, near, mid = r[p + "part"], r[p + "near"], r[p + "mid"]
        near2, mid2 = r[p + "near2"], r[p + "mid2"]
        sem = tag(p, name, c)
        if name == "c":
            kept = mid[:, self.x, :, cols] if kind == FIRST else mid[:, self.par, :, cols]
            self.came(near2.at[:, :, cols], tag(p, "x" if kind == FIRST else "p", c))
            mid2[:, :, cols] = (kept.astype(F32) + near2[:, :, cols].astype(F32)).astype(BF16)
            for d in range(1, s.zh):
                q = lax.rem(self.q + d, s.zh)
                self.send(mid2.at[q, :, cols], r[p + "far2"].at[d - 1, :, cols], sem, kv=self.across(q))
            return
        self.came(near.at[:, :, :, cols], tag(p, "p" if kind == FIRST else "x", c))
        kept = part[:, self.par, :, :, cols] if kind == FIRST else part[:, :, self.x, :, cols]
        mid[:, :, :, cols] = (kept.astype(F32) + near[:, :, :, cols].astype(F32)).astype(BF16)
        if name == "z":
            for d in range(1, s.zn):
                z = lax.rem(self.z + d, s.zn)
                src = mid.at[z // 2, lax.rem(z, 2), :, cols]
                self.send(src, r[p + "far"].at[d - 1, :, cols], sem, kv=z * 2 + self.x)
        elif name == "p":
            self.send(mid.at[:, 1 - self.par, :, cols], near2.at[:, :, cols], sem, kv=self.ppeer)
        else:
            self.send(mid.at[:, 1 - self.x, :, cols], near2.at[:, :, cols], sem, kv=self.xpeer)

    @scoped
    def sum_total(self, p, c, kind, cols):
        r = self.r
        if kind == DIRECT:
            own, far, sem = r[p + "mid"].at[self.q, self.par], r[p + "far"], tag(p, "z", c)
        else:
            own, far, sem = r[p + "mid2"].at[self.q], r[p + "far2"], tag(p, "c", c)
        total = own[:, cols].astype(F32)
        self.came(far.at[:, :, cols], sem)
        for d in range(far.shape[0]):
            total = total + far[d, :, cols].astype(F32)
        return total

    def spot(self, p, z, cols):
        return self.r[p + "hid"].at[z // 2, lax.rem(z, 2), self.x, :, cols]

    def spread_start(self, p, c, kind, cols):
        s = self.s
        mine = self.spot(p, self.z, cols)
        if kind == DIRECT:
            for d in range(1, s.zn):
                z = lax.rem(self.z + d, s.zn)
                self.send(mine, mine, tag(p, "h", c), kv=z * 2 + self.x)
        else:
            for d in range(1, s.zh):
                self.send(mine, mine, tag(p, "i", c), kv=self.across(lax.rem(self.q + d, s.zh)))

    @scoped
    def spread_step(self, p, name, c, kind, cols):
        r = self.r
        hid = r[p + "hid"]
        first = kind == FIRST
        if name == "g" and kind == DIRECT:
            self.came(r[p + "far"].at[:, :, cols], tag(p, "h", c))
        elif name == "j":
            self.came(r[p + "far2"].at[:, :, cols], tag(p, "i", c))
        elif name == "g":
            self.came(hid.at[:, 1 - self.par, self.x, :, cols], tag(p, "j", c))
        else:
            self.came(hid.at[:, self.par, 1 - self.x, :, cols], tag(p, "j", c))
        if name == "j":
            own = hid.at[:, self.par, self.x, :, cols]
            self.send(own, own, tag(p, "j", c), kv=self.xpeer if first else self.ppeer)
        elif name == "g":
            own = hid.at[:, :, self.x, :, cols]
            self.send(own, own, tag(p, "g", c), kv=self.xpeer)
        else:
            own = hid.at[:, self.par, :, :, cols]
            self.send(own, own, tag(p, "k", c), kv=self.ppeer)

    @scoped
    def spread_end(self, p, c, kind, cols):
        hid = self.r[p + "hid"]
        if kind == FIRST:
            self.came(hid.at[:, 1 - self.par, :, :, cols], tag(p, "k", c))
        else:
            self.came(hid.at[:, :, 1 - self.x, :, cols], tag(p, "g", c))
        self.need("out" if p[0] == "m" else "down" + p[0])

    @scoped
    def finish_core(self, p):
        r, s = self.r, self.s
        t0 = r[p + "t0"]
        t0[...] = r[p + "acc"][...].astype(BF16).reshape(2, s.half, s.depth)
        self.send(t0.at[1 - self.core], r[p + "t1"], p + "t", tp=self.tp + 1 - 2 * self.core)

    @scoped
    def finish_y(self, p):
        r, s = self.r, self.s
        t2 = r[p + "t2"]
        self.came(r[p + "t1"], p + "t")
        t2[...] = (r[p + "t0"][self.core].astype(F32) + r[p + "t1"][...].astype(F32)).astype(BF16)
        for d in range(1, s.ny):
            yp = lax.rem(self.y + d, s.ny)
            self.send(t2, r[p + "t3"].at[d - 1], p + "u", tp=yp * 2 + self.core)

    @scoped
    def finish_rows(self, p, weight, before):
        r, s = self.r, self.s
        t3, feat = r[p + "t3"], r[p + "feat"]
        total = r[p + "t2"][...].astype(F32)
        self.came(t3, p + "u")
        for d in range(s.ny - 1):
            total = total + t3[d].astype(F32)
        feat[self.core] = (before[self.core].astype(F32) + weight * total).astype(BF16)
        mine = feat.at[self.core]
        self.send(mine, mine, p + "v", tp=self.tp + 1 - 2 * self.core)

    @scoped
    def finish_end(self, p):
        feat = self.r[p + "feat"]
        self.came(feat.at[1 - self.core], p + "v")
        return feat

    def finish(self, p, weight, before, k):
        if k == 0:
            self.finish_core(p)
        elif k == 1:
            self.finish_y(p)
        elif k == 2:
            self.finish_rows(p, weight, before)
        else:
            self.finish_end(p)

    @scoped
    def last_start(self, p):
        r, s = self.r, self.s
        width = s.depth // s.nt
        t0, t1 = r[p + "t0"], r[p + "t1"]
        for k in range(s.nt):
            t0[k] = r[p + "acc"][:, k * width : (k + 1) * width].astype(BF16)
        for d in range(1, s.nt):
            k = lax.rem(self.tp + d, s.nt)
            self.send(t0.at[k], t1.at[d - 1], p + "t", tp=k)

    @scoped
    def last_end(self, p, weight, before, out_ref):
        r, s = self.r, self.s
        width = s.depth // s.nt
        t1 = r[p + "t1"]
        total = r[p + "t0"][self.tp].astype(F32)
        self.came(t1, p + "t")
        for d in range(s.nt - 1):
            total = total + t1[d].astype(F32)
        cols = pl.ds(pl.multiple_of(self.tp * width, LANES), width)
        mine = before[:, :, cols].astype(F32).reshape(s.rows, width)
        out_ref[:, self.part] = (mine + weight * total).reshape(s.n, s.count, width).astype(BF16)

    def finish_last(self, p, weight, before, out_ref, k):
        s = self.s
        if s.split:
            for j in (2 * k, 2 * k + 1):
                self.finish(p, weight, before, j)
            if k == 1:
                feat = self.r[p + "feat"][...].astype(F32)
                out_ref[:, self.part] = feat.reshape(s.n, s.count, s.depth).astype(BF16)
        elif k == 0:
            self.last_start(p)
        else:
            self.last_end(p, weight, before, out_ref)

    def gain(self, k):
        gains = self.r["gains"]
        return jnp.concatenate([gains[t, k : k + 1, :] for t in range(gains.shape[0])], axis=1)

    @scoped
    def normed(self, p, feat, k):
        s = self.s
        values = feat[...].astype(F32).reshape(s.rows, s.depth)
        squares = jnp.sum(values * values, axis=1, keepdims=True)
        self.r[p + "side"][...] = jnp.broadcast_to(squares, (s.rows, LANES)).reshape(s.n, s.count, LANES)
        return (values * self.gain(k)).astype(BF16)

    def put_part(self, p, lo, value):
        s = self.s
        w = value.shape[1]
        self.r[p + "part"][:, :, :, :, pl.ds(lo, w)] = value.reshape(s.zh, 2, 2, s.count, w).astype(BF16)

    def event(self, stage, c, k):
        s, r, q = self.s, self.r, self.tail
        before = (r["b" + q], r["1" + q + "feat"], r["m" + q + "feat"])
        if stage == UPDATE:
            self.update(c * s.count // UPDATES, (c + 1) * s.count // UPDATES)
        elif stage in (0, 6):
            self.feed_forward(("1" if stage == 0 else "2") + q, before[stage // 3], stage // 3, c, k)
        elif stage == 1:
            self.finish("1" + q, 0.5, before[0], k)
        elif stage == 2:
            self.project("m" + q, before[1], c, k)
        elif stage == 3:
            self.mix("m" + q)
        elif stage == 4 and c < s.groups:
            self.mixed("m" + q, c, k)
        elif stage == 5:
            self.finish("m" + q, 1.0, before[1], k)
        elif stage == 7:
            self.finish_last("2" + q, 0.5, before[2], self.outs["next"], k)

    def begin(self, p, feat, k):
        if self.stage != p:
            self.scaled, self.factor, self.lowered = self.normed(p, feat, k), None, False
            self.stage, self.started = p, 0
        self.started += 1

    @scoped
    def multiply(self, p, c):
        r = self.r
        if p[0] == "1":
            self.ready(c)
        else:
            self.need("gate2", "up2")
        _, _, lo, hi = self.s.ff_chunks[c]
        for i, w in enumerate(("gate", "up")):
            weight = r["v_" + w + p[0]]
            self.put_part(p, 2 * lo + i * (hi - lo), jnp.dot(self.scaled, weight[:, lo:hi], preferred_element_type=F32))

    def activated(self, p, c, way, cols):
        total = self.sum_total(p, c, way, cols)
        if self.factor is None:
            self.factor = self.row_factor(p)
        return total * self.factor

    @scoped
    def lower(self, p, name, c, lo, hi):
        s, r = self.s, self.r
        hidden = r[p + "hid"][:, :, :, :, pl.ds(lo, hi - lo)].astype(F32).reshape(s.rows, hi - lo)
        weight = r["v_" + name]
        value = jnp.dot(hidden.astype(BF16), weight[lo:hi, :], preferred_element_type=F32)
        if not self.lowered:
            r[p + "acc"][...] = value
        else:
            r[p + "acc"][...] += value
        self.lowered = True

    def feed_forward(self, p, feat, gain, c, k):
        chunk = self.s.ff_chunks[c]
        way, back, lo, hi = chunk
        there, home = SUM[way], SPREAD[back]
        cols, wide = self.columns(chunk), self.columns(chunk, 2)
        at = k - len(there)
        if k == 0:
            self.begin(p, feat, gain)
            self.multiply(p, c)
            self.sum_start(p, c, way, wide)
            if self.started == 2:
                self.side_send(p)
        elif at < 0:
            self.sum_step(p, there[k], c, way, wide)
        elif at == 0:
            total = self.activated(p, c, way, wide)
            hidden = sigmoid_gate(total[:, : hi - lo]) * total[:, hi - lo :]
            self.r[p + "hid"][self.q, self.par, self.x, :, cols] = hidden.astype(BF16)
            self.spread_start(p, c, back, cols)
        elif at < len(home):
            self.spread_step(p, home[at], c, back, cols)
        else:
            self.spread_end(p, c, back, cols)
            self.lower(p, "down" + p[0], c, lo, hi)

    @scoped
    def multiply_mixer(self, p, c):
        s, r = self.s, self.r
        for name, lo, hi in s.mix_chunks[c]:
            at, w = s.place[name, lo]
            weight = r["v_" + name]
            if name == "step":
                value = lax.dot_general(
                    self.scaled, weight[...], (((1,), (1,)), ((), ())), preferred_element_type=F32
                )
                self.put_part(p, at, jnp.zeros((s.rows, LANES), F32))
                self.put_part(p, at, value)
            else:
                self.put_part(p, at, jnp.dot(self.scaled, weight[:, lo:hi], preferred_element_type=F32))

    def project(self, p, feat, c, k):
        s, r = self.s, self.r
        chunk = s.mix_spans[c]
        way, _, lo, hi = chunk
        cols = self.columns(chunk)
        if k == 0:
            self.need("value", "write", "read", "step", "gate", "bias", "rate", "cw", "gg", "past")
            self.begin(p, feat, 1)
            self.multiply_mixer(p, c)
            self.sum_start(p, c, way, cols)
            if self.started == 2:
                self.side_send(p)
            if c == 2:
                self.conv_past()
        elif k < len(SUM[way]):
            self.sum_step(p, SUM[way][k], c, way, cols)
        else:
            r["proj" + self.tail][:, lo:hi] = self.activated(p, c, way, cols).astype(BF16).astype(F32)

    def mixed(self, p, g, k):
        gw = self.s.group_width
        cols = pl.ds(g * gw, gw)
        if k == 1:
            self.spread_step(p, "g", g, DIRECT, cols)
        else:
            self.spread_end(p, g, DIRECT, cols)
            self.lower(p, "out", g, g * gw, (g + 1) * gw)

    @scoped
    def mix(self, p):
        s, r, q = self.s, self.r, self.tail
        base = self.part * s.count
        proj, fresh_ref = r["proj" + q], self.outs["fresh"]
        self.lowered = False

        def take(name):
            pieces = []
            for chunk in s.mix_chunks:
                for other, lo, _ in chunk:
                    if other == name:
                        pieces.append((lo, *s.place[name, lo]))
            return jnp.concatenate([proj[:, at : at + w] for _, at, w in sorted(pieces)], axis=1)

        values, writes, reads = take("value"), take("write"), take("read")
        at, _ = s.place["step", 0]
        steps = proj[:, at : at + LANES][:, : s.heads]
        step = jax.nn.softplus(steps + r["v_bias"][...])
        decay = jnp.exp(-step * jnp.exp(r["v_rate"][...]))
        head_row = lax.broadcasted_iota(jnp.int32, (s.heads, s.inner), 0)
        head_col = lax.broadcasted_iota(jnp.int32, (s.heads, s.inner), 1) // s.head
        widen = (head_row == head_col).astype(F32)
        exact = dict(preferred_element_type=F32, precision=lax.Precision.HIGHEST)
        step_wide = jnp.dot(step, widen, **exact)
        decay_wide = jnp.dot(decay, widen, **exact)
        r["decay" + q][...] = decay
        gw, st = s.group_width, s.state
        conv_w = r["v_cw"]
        taps = conv_w.shape[0]
        gates = take("gate")
        scaled_inputs, lone, activated = [], [], []
        for g in range(s.groups):
            fresh = jnp.concatenate(
                [values[:, g * gw : (g + 1) * gw], writes[:, g * st : (g + 1) * st], reads[:, g * st : (g + 1) * st]],
                axis=1,
            )
            fresh_ref[g, base : base + s.count, :] = fresh
            act = sigmoid_gate(r["conv" + q][g] + fresh * conv_w[taps - 1, g : g + 1, :])
            inputs, write, read = act[:, :gw], act[:, gw : gw + st], act[:, gw + st :]
            si = inputs * step_wide[:, g * gw : (g + 1) * gw]
            r["write" + q][g] = write
            r["vecs" + q][g] = read
            scaled_inputs.append(si)
            lone.append(jnp.sum(write * read, axis=1, keepdims=True))
        state = r["v_state"]
        per = s.heads // s.groups
        row = lax.broadcasted_iota(jnp.int32, (s.count, s.state), 0)
        self.need("state")

        def one(k, totals):
            found = []
            for g, total in enumerate(totals):
                held = state[base + k, g * per : (g + 1) * per].reshape(gw, st).astype(BF16)
                vec = jnp.where(row == k, r["vecs" + q][g], 0.0).astype(BF16)
                drawn = lax.dot_general(vec, held, (((1,), (1,)), ((), ())), preferred_element_type=F32)
                found.append(total + drawn)
            return tuple(found)

        drawn = lax.fori_loop(
            0, s.count, one, tuple(jnp.zeros((s.count, gw), F32) for _ in range(s.groups)), unroll=4
        )
        whole = [pl.ds(g * gw, gw) for g in range(s.groups)]
        for g in range(s.groups):
            cols = slice(g * gw, (g + 1) * gw)
            readout = decay_wide[:, cols] * drawn[g] + scaled_inputs[g] * lone[g]
            gated = readout * sigmoid_gate(gates[:, cols])
            mean = jnp.sum(gated * gated, axis=1, keepdims=True) / gw
            mixed = gated * lax.rsqrt(mean + norm_epsilon) * r["v_gg"][:, cols]
            r[p + "hid"][self.q, self.par, self.x, :, whole[g]] = mixed.astype(BF16)
            self.spread_start(p, g, DIRECT, whole[g])
        for g in range(s.groups):
            si = scaled_inputs[g]
            high = si.astype(BF16).astype(F32)
            fill = jnp.zeros((s.deep - 3 * s.count, gw), F32)
            r["left" + q][g] = jnp.concatenate([high, high, si - high, fill], axis=0).T.astype(BF16)

    @scoped
    def update(self, lo, hi):
        s, r = self.s, self.r
        q, first = self.tail, self.part * s.count
        state, left, gw, st = r["v_state"], r["left" + q], s.group_width, s.state
        per, block = s.heads // s.groups, 2
        row = lax.broadcasted_iota(jnp.int32, (s.count, st), 0)

        def one(j, carry):
            base = j * block
            for g in range(s.groups):
                write = r["write" + q][g]
                picked = jnp.concatenate([jnp.where(row == base + i, write, 0.0) for i in range(block)], axis=1)
                high = picked.astype(BF16).astype(F32)
                fill = jnp.zeros((s.deep - 3 * s.count, block * st), F32)
                right = jnp.concatenate([high, picked - high, high, fill], axis=0).astype(BF16)
                outer = jnp.dot(left[g], right, preferred_element_type=F32)
                for i in range(block):
                    decay = r["decay" + q][pl.ds(base + i, 1), :]
                    for h in range(g * per, (g + 1) * per):
                        at = (h - g * per) * s.head
                        new = outer[at : at + s.head, i * st : (i + 1) * st]
                        state[first + base + i, h] = state[first + base + i, h] * decay[:, h : h + 1] + new
            return carry

        lax.fori_loop(lo // block, hi // block, one, 0)

    @scoped
    def conv_past(self):
        s, r = self.s, self.r
        past, weight, conv = r["v_past"], r["v_cw"], r["conv" + self.tail]
        first = self.part * s.count
        taps = weight.shape[0]

        def one(k, carry):
            total = past[first + k, 0].astype(F32) * weight[0]
            for t in range(1, taps - 1):
                total = total + past[first + k, t].astype(F32) * weight[t]
            for g in range(s.groups):
                conv[g, pl.ds(k, 1), :] = total[g : g + 1, :]
            return carry

        lax.fori_loop(0, s.count, one, 0)


def step_kernel(s, plan, names, *refs):
    count = len(names)
    hbm = dict(zip(names, refs[:count]))
    outs = dict(zip(("next", "fresh", "state"), refs[count : count + 3]))
    r = dict(zip(plan.names, refs[count + 3 :]))
    r["v_state"] = outs["state"]
    sent = []
    bodies = [Body(s, r, part, sent) for part in range(s.parts)]
    body = bodies[0]
    order = [n for n in names if n not in ("stream", "gain1", "gain2", "gain3")]
    gains = r["gains"]
    width = s.depth // s.nt
    head = []
    if s.split:
        head.append(body.local(hbm["stream"], r["feat"], r["l0"].at[0]))
        head.append(body.local(hbm["gain1"], gains.at[0], r["l0"].at[1]))
    else:
        mine = pl.ds(pl.multiple_of(body.tp * width, LANES), width)
        head.append(body.local(hbm["stream"], r["feat"].at[:, :, :, mine], r["l0"].at[0]))
        for k in range(3):
            head.append(body.local(hbm["gain%d" % (k + 1)], gains.at[body.tp, pl.ds(k, 1)], r["l0"].at[k + 1]))
    sem = pltpu.get_barrier_semaphore()
    for d in range(1, s.n):
        pl.semaphore_signal(sem, inc=1, device_id={KV: lax.rem(body.me + d, s.n)}, device_id_type=MESH)
    for d in range(1, s.nt):
        pl.semaphore_signal(sem, inc=1, device_id={TP: lax.rem(body.tp + d, s.nt)}, device_id_type=MESH)
    for copy in head:
        copy.wait()
    first = {}
    for c in range(len(s.ff_chunks)):
        cols = body.columns(s.ff_chunks[c])
        for i, name in enumerate(("gate1", "up1")):
            first[c, i] = body.local(hbm[name].at[:, cols], r["v_" + name].at[:, cols], r["w1"].at[i, c])
    pl.semaphore_wait(sem, s.n + s.nt - 2)
    if not s.split:
        block = r["feat"].at[:, :, :, mine]
        for d in range(1, s.nt):
            k = lax.rem(body.tp + d, s.nt)
            body.send(block, block, "f", tp=k)
            body.send(gains.at[body.tp], gains.at[body.tp], "n", tp=k)
        body.came(r["feat"].at[:, :, :, pl.ds(0, (s.nt - 1) * width)], "f")
        body.came(gains.at[pl.ds(0, s.nt - 1)], "n")
    rest = {}
    begun = set()

    def ready(c):
        if c in begun:
            return
        first[c, 0].wait()
        first[c, 1].wait()
        if not begun:
            for i, name in enumerate(order):
                if name not in ("gate1", "up1"):
                    rest[name] = body.local(hbm[name], r["v_" + name], r["w"].at[i])
        begun.add(c)

    waited = set()

    def need(*wanted):
        for name in wanted:
            if name not in waited:
                waited.add(name)
                rest[name].wait()

    for body in bodies:
        body.need, body.ready, body.outs = need, ready, outs
        rows = r["feat"][:, body.part].astype(F32)
        r["b" + body.tail][...] = rows.reshape(2, s.half, s.depth).astype(BF16)
    for code in ORDER:
        bodies[code // 10000].event(code // 1000 % 10, code // 10 % 100, code % 10)
    for copy in sent:
        copy.wait_send()


def write_kernel(s, blocks, past_ref, fresh_ref, next_ref, state_ref, state_out, past_out, next_out, sem):
    taps = past_ref.shape[1]
    count = past_ref.shape[0]
    step = count // blocks
    copies = []
    for k in range(blocks):
        rows = pl.ds(k * step, step)
        copy = pltpu.make_async_copy(state_ref.at[rows], state_out.at[rows], sem.at[k])
        copy.start()
        copies.append(copy)
    next_out[...] = next_ref[...]

    def one(k, carry):
        for t in range(taps - 1):
            past_out[k, t] = past_ref[k, t + 1]
        newest = [fresh_ref[g, pl.ds(k, 1), :] for g in range(s.groups)]
        past_out[k, taps - 1] = jnp.concatenate(newest, axis=0).astype(BF16)
        return carry

    lax.fori_loop(0, count, one, 0)
    for copy in copies:
        copy.wait()


def gathered(stream, gains):
    n = lax.axis_size(TP)
    features = lax.all_gather(stream, TP, axis=1, tiled=True)
    packed = lax.all_gather(jnp.stack(gains), TP, axis=1, tiled=True)
    return features, packed


def on_device(
    stream,
    ssm_state,
    constate,
    first_gain,
    first_gate,
    first_up,
    first_down,
    mix_gain,
    gate_in,
    value_in,
    write_in,
    read_in,
    step_in,
    conv_weight,
    step_bias,
    log_decay_rate,
    group_gain,
    out_weight,
    last_norm_gain,
    second_gate,
    second_up,
    second_down,
):
    n, nt = lax.axis_size(KV), lax.axis_size(TP)
    rows, width = stream.shape
    depth, units = first_gate.shape
    heads, head, state = ssm_state.shape[1:]
    groups = conv_weight.shape[1]
    split = width % LANES != 0
    s = Sizes(n, nt, rows, depth, units, heads, head, state, groups, split)
    if split:
        features, packed = gathered(stream, [first_gain, mix_gain, last_norm_gain])
        named = {"stream": features.reshape(n, s.parts, s.count, depth), "gain1": packed}
    else:
        named = {
            "stream": stream.reshape(n, s.parts, s.count, width),
            "gain1": first_gain[None],
            "gain2": mix_gain[None],
            "gain3": last_norm_gain[None],
        }
    weights = {
        "gate1": first_gate,
        "up1": first_up,
        "down1": first_down,
        "value": value_in,
        "gate": gate_in,
        "write": write_in,
        "read": read_in,
        "step": step_in.T,
        "cw": conv_weight,
        "bias": step_bias[None],
        "rate": log_decay_rate[None],
        "gg": group_gain[None],
        "past": constate,
        "state": ssm_state,
        "out": out_weight,
        "gate2": second_gate,
        "up2": second_up,
        "down2": second_down,
    }
    plan = make_plan(s, [(k, v.shape, v.dtype) for k, v in weights.items()])
    named.update(weights)
    result, fresh, held = pl.pallas_call(
        functools.partial(step_kernel, s, plan, list(named)),
        out_shape=[
            pltpu.VMEM((n, s.parts, s.count, depth if split else width), BF16),
            pltpu.VMEM((groups, rows // n, s.channels), F32),
            pltpu.VMEM(ssm_state.shape, ssm_state.dtype),
        ],
        in_specs=[HB] * len(named),
        out_specs=[VM] * 3,
        scratch_shapes=plan.shapes,
        compiler_params=pltpu.CompilerParams(
            collective_id=0, has_side_effects=True, vmem_limit_bytes=48 * 1024 * 1024
        ),
    )(*named.values())
    if split:
        me = lax.axis_index(TP)
        result = lax.dynamic_slice_in_dim(result, me * width, width, axis=3)
    blocks = 8
    state_next, past_next, stream_next = pl.pallas_call(
        functools.partial(write_kernel, s, blocks),
        out_shape=[
            jax.ShapeDtypeStruct(ssm_state.shape, ssm_state.dtype),
            jax.ShapeDtypeStruct(constate.shape, constate.dtype),
            jax.ShapeDtypeStruct(result.shape, BF16),
        ],
        in_specs=[VM] * 4,
        out_specs=[HB, VM, VM],
        scratch_shapes=[pltpu.SemaphoreType.DMA((blocks,))],
        compiler_params=pltpu.CompilerParams(vmem_limit_bytes=8 * 1024 * 1024),
    )(constate, fresh, result, held)
    return (stream_next.reshape(stream.shape), state_next, past_next)


def solution(mesh):
    return jax.shard_map(
        on_device,
        mesh=mesh,
        in_specs=(
            P(None, (KV, TP)),
            P(KV, TP, None, None),
            P(KV, None, TP, None),
            P((KV, TP)),
            P(KV, TP),
            P(KV, TP),
            P(TP, KV),
            P((KV, TP)),
            P(KV, TP),
            P(KV, TP),
            P(KV, TP),
            P(KV, TP),
            P(KV, TP),
            P(None, TP, None),
            P(TP),
            P(TP),
            P(TP),
            P(TP, KV),
            P((KV, TP)),
            P(KV, TP),
            P(KV, TP),
            P(TP, KV),
        ),
        out_specs=(P(None, (KV, TP)), P(KV, TP, None, None), P(KV, None, TP, None)),
        check_vma=False,
    )
```

```python
import functools

import jax
import jax.numpy as jnp
from jax import lax
from jax.experimental import pallas as pl
from jax.experimental.pallas import tpu as pltpu
from jax.sharding import PartitionSpec as P

norm_epsilon = 1e-06
MESH = pl.DeviceIdType.MESH
LANES = 128
KV, TP = "kv", "tp"
DIRECT, THREE, FIRST = "d", "t", "f"
VM = pl.BlockSpec(memory_space=pltpu.VMEM)
HB = pl.BlockSpec(memory_space=pltpu.HBM)
F32 = jnp.float32
BF16 = jnp.bfloat16


def sigmoid_gate(v):
    return v / (1.0 + jnp.exp(-v))


def copy_to(src, dst, send, recv, **where):
    return pltpu.make_async_remote_copy(
        src_ref=src, dst_ref=dst, send_sem=send, recv_sem=recv, device_id=where, device_id_type=MESH
    )


def tag(p, stage, c):
    return p + stage + str(c)


class Plan:
    def __init__(self):
        self.names, self.shapes = [], []

    def add(self, name, shape, dtype):
        self.names.append(name)
        self.shapes.append(pltpu.VMEM(shape, dtype))

    def sem(self, name, *shape):
        self.names.append(name)
        self.shapes.append(pltpu.SemaphoreType.DMA(shape or (1,)))


def cut(total, shares):
    ends = [0] + [max(1, round(total * s)) for s in shares] + [total]
    return [(a, b) for a, b in zip(ends, ends[1:]) if b > a]


SUM = {DIRECT: "xz", THREE: "xpc", FIRST: "pxc"}
SPREAD = {DIRECT: "hg", THREE: "ijg", FIRST: "ijk"}
FF_CHUNKS = [(DIRECT, THREE, 4), (FIRST, FIRST, 6), (THREE, DIRECT, 6), (THREE, DIRECT, 6)]
MIX_WAYS = (DIRECT, FIRST, DIRECT, DIRECT)
PARTS, UPDATE, UPDATES = 2, 8, 4
ORDER = [
    0, 10, 20, 30, 1, 11, 10010, 10000, 21, 10020, 2, 31, 12, 10030,
    22, 10011, 10001, 32, 10021, 3, 13, 23, 10002, 10031, 10012, 33, 4, 10022,
    14, 10032, 24, 10003, 5, 10013, 15, 34, 10023, 10004, 25, 10033, 10014, 16,
    35, 1000, 10024, 10034, 10015, 1001, 10005, 10025, 1002, 10035, 10016, 11000, 2000, 2020,
    2010, 2030, 11001, 2001, 2011, 2021, 11002, 12010, 12000, 12020, 2031, 2012, 12011, 2002,
    2022, 12030, 12021, 12001, 2032, 2013, 3000, 12031, 8030, 8010, 8000, 12012, 4001, 12022,
    4011, 12002, 12013, 12032, 13000, 4002, 4012, 5000, 14001, 18000, 14011, 5001, 5002, 6000,
    6020, 14002, 6010, 14012, 15000, 6030, 6001, 15001, 6021, 6011, 15002, 16010, 16000, 16020,
    8020, 16030, 6002, 6031, 6012, 6022, 16001, 6003, 6032, 16011, 16021, 18010, 18020, 18030,
    6023, 6013, 16002, 16031, 16012, 6004, 6033, 16022, 6014, 16032, 16003, 6024, 16013, 16023,
    16004, 16033, 16014, 6034, 6005, 16024, 6015, 16015, 16034, 6025, 16005, 16025, 6016, 6035,
    7000, 16016, 16035, 17000, 7001, 17001,
]


class Sizes:
    def __init__(self, n, nt, rows, depth, units, heads, head, state, groups, split):
        self.n, self.nt, self.rows, self.depth, self.units = n, nt, rows, depth, units
        self.heads, self.head, self.state, self.groups, self.split = heads, head, state, groups, split
        self.zn, self.zh, self.ny = n // 2, n // 4, nt // 2
        self.parts = PARTS
        self.all_rows, self.rows = rows, rows // PARTS
        self.count = self.rows // n
        self.deep = -(-3 * self.count // LANES) * LANES
        tiles = units // LANES
        shares = [share for _, _, share in FF_CHUNKS]
        ends = [sum(shares[: i + 1]) / sum(shares) for i in range(len(shares) - 1)]
        self.ff_chunks = [
            (out, back, a * LANES, z * LANES) for (out, back, _), (a, z) in zip(FF_CHUNKS, cut(tiles, ends))
        ]
        self.inner = heads * head
        self.group_width = self.inner // groups
        self.channels = self.group_width + 2 * state
        v = self.inner // LANES
        vec = groups * state
        gb = max(1, v * 5 // 8)
        self.mix_chunks = [
            [("value", 0, v // 2 * LANES)],
            [("gate", 0, gb * LANES)],
            [("value", v // 2 * LANES, v * LANES), ("write", 0, vec)],
            [("read", 0, vec), ("step", 0, LANES), ("gate", gb * LANES, v * LANES)],
        ]
        spans, at = [], 0
        self.place = {}
        for chunk in self.mix_chunks:
            lo = at
            for name, a, z in chunk:
                self.place[name, a] = (at, z - a)
                at += z - a
            spans.append((lo, at))
        self.mix_spans = [(way, None, a, z) for way, (a, z) in zip(MIX_WAYS, spans)]
        self.mix_width = at


def add_sum(plan, s, p, width, chunks):
    zn, zh, cnt, n = s.zn, s.zh, s.count, s.n
    zl = max(1, zh - 1)
    plan.add(p + "part", (zh, 2, 2, cnt, width), BF16)
    plan.add(p + "near", (zh, 2, cnt, width), BF16)
    plan.add(p + "mid", (zh, 2, cnt, width), BF16)
    plan.add(p + "far", (zn - 1, cnt, width), BF16)
    plan.add(p + "near2", (zh, cnt, width), BF16)
    plan.add(p + "mid2", (zh, cnt, width), BF16)
    plan.add(p + "far2", (zl, cnt, width), BF16)
    plan.add(p + "side", (n, s.count, LANES), F32)
    plan.add(p + "sides", (n - 1, s.count, LANES), F32)
    plan.sem(p + "e")
    for c, chunk in enumerate(chunks):
        for stage in SUM[chunk[0]]:
            plan.sem(p + stage + str(c))


def add_spread(plan, s, p, width, chunks):
    plan.add(p + "hid", (s.zh, 2, 2, s.count, width), BF16)
    for c, chunk in enumerate(chunks):
        for stage in SPREAD[chunk[1]]:
            plan.sem(p + stage + str(c))


def add_finish(plan, s, p, last):
    plan.add(p + "acc", (s.rows, s.depth), F32)
    if last and not s.split:
        plan.add(p + "t0", (s.nt, s.rows, s.depth // s.nt), BF16)
        plan.add(p + "t1", (s.nt - 1, s.rows, s.depth // s.nt), BF16)
        plan.sem(p + "t")
        return
    for name in ("t0", "t1", "t2", "feat"):
        plan.add(p + name, (s.rows, s.depth), BF16)
    plan.add(p + "t3", (max(1, s.ny - 1), s.rows, s.depth), BF16)
    for stage in "uv":
        plan.sem(p + stage)


def make_plan(s, weights):
    plan = Plan()
    for name, shape, dtype in weights:
        if name != "state":
            plan.add("v_" + name, shape, dtype)
    plan.sem("w", len(weights))
    plan.sem("w1", 2, len(s.ff_chunks))
    plan.add("feat", (s.n, s.parts, s.count, s.depth), BF16)
    plan.add("gains", (s.nt, 3, s.depth // s.nt) if not s.split else (1, 3, s.depth), F32)
    plan.sem("l0", 4)
    plan.sem("sent")
    plan.sem("f", s.parts)
    plan.sem("n")
    for part in range(s.parts):
        q = str(part)
        plan.add("b" + q, (s.rows, s.depth), BF16)
        for p in ("1" + q, "2" + q):
            add_sum(plan, s, p, 2 * s.units, s.ff_chunks)
            add_spread(plan, s, p, s.units, s.ff_chunks)
        add_sum(plan, s, "m" + q, s.mix_width, s.mix_spans)
        add_spread(plan, s, "m" + q, s.inner, [(DIRECT, DIRECT)] * s.groups)
        add_finish(plan, s, "1" + q, False)
        add_finish(plan, s, "m" + q, False)
        add_finish(plan, s, "2" + q, True)
        plan.add("proj" + q, (s.count, s.mix_width), F32)
        plan.add("conv" + q, (s.groups, s.count, s.channels), F32)
        plan.add("vecs" + q, (s.groups, s.count, s.state), F32)
        plan.add("left" + q, (s.groups, s.group_width, s.deep), BF16)
        plan.add("write" + q, (s.groups, s.count, s.state), F32)
        plan.add("decay" + q, (s.count, s.heads), F32)
    return plan


def scoped(f):
    @functools.wraps(f)
    def inner(*args):
        tag = "_".join(str(a) for a in args if isinstance(a, (str, int)))
        with jax.named_scope(f.__name__ + "_" + tag):
            return f(*args)

    return inner


class Body:
    def __init__(self, s, r, part, sent):
        self.s, self.r, self.sent, self.part, self.tail = s, r, sent, part, str(part)
        self.stage = None
        me = lax.axis_index(KV)
        self.me, self.z, self.x = me, me // 2, lax.rem(me, 2)
        self.q, self.par = me // 4, lax.rem(me // 2, 2)
        self.tp = lax.axis_index(TP)
        self.y, self.core = self.tp // 2, lax.rem(self.tp, 2)
        self.xpeer = self.z * 2 + 1 - self.x
        self.ppeer = (self.q * 2 + 1 - self.par) * 2 + self.x

    def start(self, copy):
        copy.start()
        self.sent.append(copy)
        return copy

    def send(self, src, dst, sem, **where):
        return self.start(copy_to(src, dst, self.r["sent"].at[0], self.r[sem].at[0], **where))

    def came(self, place, sem):
        pltpu.make_async_copy(place, place, self.r[sem].at[0]).wait()

    def local(self, src, dst, sem):
        copy = pltpu.make_async_copy(src, dst, sem)
        copy.start()
        return copy

    @scoped
    def side_send(self, p):
        side, sides = self.r[p + "side"], self.r[p + "sides"]
        for d in range(1, self.s.n):
            k = lax.rem(self.me + d, self.s.n)
            self.send(side.at[k], sides.at[d - 1], p + "e", kv=k)

    @scoped
    def row_factor(self, p):
        s = self.s
        total = self.r[p + "side"][self.me]
        self.came(self.r[p + "sides"], p + "e")
        for d in range(s.n - 1):
            total = total + self.r[p + "sides"][d]
        return lax.rsqrt(total / (s.depth * s.n) + norm_epsilon)[:, :1]

    def columns(self, chunk, scale=1):
        return pl.ds(chunk[2] * scale, (chunk[3] - chunk[2]) * scale)

    def across(self, q):
        return (q * 2 + self.par) * 2 + self.x

    def sum_start(self, p, c, kind, cols):
        part, near = self.r[p + "part"], self.r[p + "near"].at[:, :, :, cols]
        if kind == FIRST:
            self.send(part.at[:, 1 - self.par, :, :, cols], near, tag(p, "p", c), kv=self.ppeer)
        else:
            self.send(part.at[:, :, 1 - self.x, :, cols], near, tag(p, "x", c), kv=self.xpeer)

    @scoped
    def sum_step(self, p, name, c, kind, cols):
        r, s = self.r, self.s
        part, near, mid = r[p + "part"], r[p + "near"], r[p + "mid"]
        near2, mid2 = r[p + "near2"], r[p + "mid2"]
        sem = tag(p, name, c)
        if name == "c":
            kept = mid[:, self.x, :, cols] if kind == FIRST else mid[:, self.par, :, cols]
            self.came(near2.at[:, :, cols], tag(p, "x" if kind == FIRST else "p", c))
            mid2[:, :, cols] = (kept.astype(F32) + near2[:, :, cols].astype(F32)).astype(BF16)
            for d in range(1, s.zh):
                q = lax.rem(self.q + d, s.zh)
                self.send(mid2.at[q, :, cols], r[p + "far2"].at[d - 1, :, cols], sem, kv=self.across(q))
            return
        self.came(near.at[:, :, :, cols], tag(p, "p" if kind == FIRST else "x", c))
        kept = part[:, self.par, :, :, cols] if kind == FIRST else part[:, :, self.x, :, cols]
        mid[:, :, :, cols] = (kept.astype(F32) + near[:, :, :, cols].astype(F32)).astype(BF16)
        if name == "z":
            for d in range(1, s.zn):
                z = lax.rem(self.z + d, s.zn)
                src = mid.at[z // 2, lax.rem(z, 2), :, cols]
                self.send(src, r[p + "far"].at[d - 1, :, cols], sem, kv=z * 2 + self.x)
        elif name == "p":
            self.send(mid.at[:, 1 - self.par, :, cols], near2.at[:, :, cols], sem, kv=self.ppeer)
        else:
            self.send(mid.at[:, 1 - self.x, :, cols], near2.at[:, :, cols], sem, kv=self.xpeer)

    @scoped
    def sum_total(self, p, c, kind, cols):
        r = self.r
        if kind == DIRECT:
            own, far, sem = r[p + "mid"].at[self.q, self.par], r[p + "far"], tag(p, "z", c)
        else:
            own, far, sem = r[p + "mid2"].at[self.q], r[p + "far2"], tag(p, "c", c)
        total = own[:, cols].astype(F32)
        self.came(far.at[:, :, cols], sem)
        for d in range(far.shape[0]):
            total = total + far[d, :, cols].astype(F32)
        return total

    def spot(self, p, z, cols):
        return self.r[p + "hid"].at[z // 2, lax.rem(z, 2), self.x, :, cols]

    def spread_start(self, p, c, kind, cols):
        s = self.s
        mine = self.spot(p, self.z, cols)
        if kind == DIRECT:
            for d in range(1, s.zn):
                z = lax.rem(self.z + d, s.zn)
                self.send(mine, mine, tag(p, "h", c), kv=z * 2 + self.x)
        else:
            for d in range(1, s.zh):
                self.send(mine, mine, tag(p, "i", c), kv=self.across(lax.rem(self.q + d, s.zh)))

    @scoped
    def spread_step(self, p, name, c, kind, cols):
        r = self.r
        hid = r[p + "hid"]
        first = kind == FIRST
        if name == "g" and kind == DIRECT:
            self.came(r[p + "far"].at[:, :, cols], tag(p, "h", c))
        elif name == "j":
            self.came(r[p + "far2"].at[:, :, cols], tag(p, "i", c))
        elif name == "g":
            self.came(hid.at[:, 1 - self.par, self.x, :, cols], tag(p, "j", c))
        else:
            self.came(hid.at[:, self.par, 1 - self.x, :, cols], tag(p, "j", c))
        if name == "j":
            own = hid.at[:, self.par, self.x, :, cols]
            self.send(own, own, tag(p, "j", c), kv=self.xpeer if first else self.ppeer)
        elif name == "g":
            own = hid.at[:, :, self.x, :, cols]
            self.send(own, own, tag(p, "g", c), kv=self.xpeer)
        else:
            own = hid.at[:, self.par, :, :, cols]
            self.send(own, own, tag(p, "k", c), kv=self.ppeer)

    @scoped
    def spread_end(self, p, c, kind, cols):
        hid = self.r[p + "hid"]
        if kind == FIRST:
            self.came(hid.at[:, 1 - self.par, :, :, cols], tag(p, "k", c))
        else:
            self.came(hid.at[:, :, 1 - self.x, :, cols], tag(p, "g", c))
        self.need("out" if p[0] == "m" else "down" + p[0])

    @scoped
    def finish(self, p, weight, before, k):
        r, s = self.r, self.s
        t0, t1, t2, t3, feat = (r[p + name] for name in ("t0", "t1", "t2", "t3", "feat"))
        if k == 0:
            t0[...] = r[p + "acc"][...].astype(BF16)
            for d in range(1, s.ny):
                yp = lax.rem(self.y + d, s.ny)
                self.send(t0, t3.at[d - 1], p + "u", tp=yp * 2 + self.core)
        elif k == 1:
            total = t0[...].astype(F32)
            self.came(t3, p + "u")
            for d in range(s.ny - 1):
                total = total + t3[d].astype(F32)
            t2[...] = total.astype(BF16)
            self.send(t2, t1, p + "v", tp=self.tp + 1 - 2 * self.core)
        else:
            self.came(t1, p + "v")
            total = t2[...].astype(F32) + t1[...].astype(F32)
            feat[...] = (before[...].astype(F32) + weight * total).astype(BF16)

    @scoped
    def last_start(self, p):
        r, s = self.r, self.s
        width = s.depth // s.nt
        t0, t1 = r[p + "t0"], r[p + "t1"]
        for k in range(s.nt):
            t0[k] = r[p + "acc"][:, k * width : (k + 1) * width].astype(BF16)
        for d in range(1, s.nt):
            k = lax.rem(self.tp + d, s.nt)
            self.send(t0.at[k], t1.at[d - 1], p + "t", tp=k)

    @scoped
    def last_end(self, p, weight, before, out_ref):
        r, s = self.r, self.s
        width = s.depth // s.nt
        t1 = r[p + "t1"]
        total = r[p + "t0"][self.tp].astype(F32)
        self.came(t1, p + "t")
        for d in range(s.nt - 1):
            total = total + t1[d].astype(F32)
        cols = pl.ds(pl.multiple_of(self.tp * width, LANES), width)
        mine = before[:, cols].astype(F32)
        out_ref[:, self.part] = (mine + weight * total).reshape(s.n, s.count, width).astype(BF16)

    def finish_last(self, p, weight, before, out_ref, k):
        s = self.s
        if s.split:
            for j in ((0,), (1, 2))[k]:
                self.finish(p, weight, before, j)
            if k == 1:
                feat = self.r[p + "feat"][...].astype(F32)
                out_ref[:, self.part] = feat.reshape(s.n, s.count, s.depth).astype(BF16)
        elif k == 0:
            self.last_start(p)
        else:
            self.last_end(p, weight, before, out_ref)

    def gain(self, k):
        gains = self.r["gains"]
        return jnp.concatenate([gains[t, k : k + 1, :] for t in range(gains.shape[0])], axis=1)

    @scoped
    def normed(self, p, feat, k):
        s = self.s
        values = feat[...].astype(F32)
        squares = jnp.sum(values * values, axis=1, keepdims=True)
        self.r[p + "side"][...] = jnp.broadcast_to(squares, (s.rows, LANES)).reshape(s.n, s.count, LANES)
        return (values * self.gain(k)).astype(BF16)

    def put_part(self, p, lo, value):
        s = self.s
        w = value.shape[1]
        self.r[p + "part"][:, :, :, :, pl.ds(lo, w)] = value.reshape(s.zh, 2, 2, s.count, w).astype(BF16)

    def event(self, stage, c, k):
        s, r, q = self.s, self.r, self.tail
        before = (r["b" + q], r["1" + q + "feat"], r["m" + q + "feat"])
        if stage == UPDATE:
            self.update(c * s.count // UPDATES, (c + 1) * s.count // UPDATES)
        elif stage in (0, 6):
            self.feed_forward(("1" if stage == 0 else "2") + q, before[stage // 3], stage // 3, c, k)
        elif stage == 1:
            self.finish("1" + q, 0.5, before[0], k)
        elif stage == 2:
            self.project("m" + q, before[1], c, k)
        elif stage == 3:
            self.mix("m" + q)
        elif stage == 4 and c < s.groups:
            self.mixed("m" + q, c, k)
        elif stage == 5:
            self.finish("m" + q, 1.0, before[1], k)
        elif stage == 7:
            self.finish_last("2" + q, 0.5, before[2], self.outs["next"], k)

    def begin(self, p, feat, k):
        if self.stage is None:
            self.arrive(self.part)
        if self.stage != p:
            self.scaled, self.factor, self.lowered = self.normed(p, feat, k), None, False
            self.stage, self.started = p, 0
        self.started += 1

    @scoped
    def multiply(self, p, c):
        r = self.r
        if p[0] == "1":
            self.ready(c)
        else:
            self.need("gate2", "up2")
        _, _, lo, hi = self.s.ff_chunks[c]
        for i, w in enumerate(("gate", "up")):
            weight = r["v_" + w + p[0]]
            self.put_part(p, 2 * lo + i * (hi - lo), jnp.dot(self.scaled, weight[:, lo:hi], preferred_element_type=F32))

    def activated(self, p, c, way, cols):
        total = self.sum_total(p, c, way, cols)
        if self.factor is None:
            self.factor = self.row_factor(p)
        return total * self.factor

    @scoped
    def lower(self, p, name, c, lo, hi):
        s, r = self.s, self.r
        hidden = r[p + "hid"][:, :, :, :, pl.ds(lo, hi - lo)].astype(F32).reshape(s.rows, hi - lo)
        weight = r["v_" + name]
        value = jnp.dot(hidden.astype(BF16), weight[lo:hi, :], preferred_element_type=F32)
        if not self.lowered:
            r[p + "acc"][...] = value
        else:
            r[p + "acc"][...] += value
        self.lowered = True

    def feed_forward(self, p, feat, gain, c, k):
        chunk = self.s.ff_chunks[c]
        way, back, lo, hi = chunk
        there, home = SUM[way], SPREAD[back]
        cols, wide = self.columns(chunk), self.columns(chunk, 2)
        at = k - len(there)
        if k == 0:
            self.begin(p, feat, gain)
            self.multiply(p, c)
            self.sum_start(p, c, way, wide)
            if self.started == 2:
                self.side_send(p)
        elif at < 0:
            self.sum_step(p, there[k], c, way, wide)
        elif at == 0:
            total = self.activated(p, c, way, wide)
            hidden = sigmoid_gate(total[:, : hi - lo]) * total[:, hi - lo :]
            self.r[p + "hid"][self.q, self.par, self.x, :, cols] = hidden.astype(BF16)
            self.spread_start(p, c, back, cols)
        elif at < len(home):
            self.spread_step(p, home[at], c, back, cols)
        else:
            self.spread_end(p, c, back, cols)
            self.lower(p, "down" + p[0], c, lo, hi)

    @scoped
    def multiply_mixer(self, p, c):
        s, r = self.s, self.r
        for name, lo, hi in s.mix_chunks[c]:
            at, w = s.place[name, lo]
            weight = r["v_" + name]
            if name == "step":
                value = lax.dot_general(
                    self.scaled, weight[...], (((1,), (1,)), ((), ())), preferred_element_type=F32
                )
                self.put_part(p, at, jnp.zeros((s.rows, LANES), F32))
                self.put_part(p, at, value)
            else:
                self.put_part(p, at, jnp.dot(self.scaled, weight[:, lo:hi], preferred_element_type=F32))

    def project(self, p, feat, c, k):
        s, r = self.s, self.r
        chunk = s.mix_spans[c]
        way, _, lo, hi = chunk
        cols = self.columns(chunk)
        if k == 0:
            self.need("value", "write", "read", "step", "gate", "bias", "rate", "cw", "gg", "past")
            self.begin(p, feat, 1)
            self.multiply_mixer(p, c)
            self.sum_start(p, c, way, cols)
            if self.started == 2:
                self.side_send(p)
            if c == 2:
                self.conv_past()
        elif k < len(SUM[way]):
            self.sum_step(p, SUM[way][k], c, way, cols)
        else:
            r["proj" + self.tail][:, lo:hi] = self.activated(p, c, way, cols).astype(BF16).astype(F32)

    def mixed(self, p, g, k):
        gw = self.s.group_width
        cols = pl.ds(g * gw, gw)
        if k == 1:
            self.spread_step(p, "g", g, DIRECT, cols)
        else:
            self.spread_end(p, g, DIRECT, cols)
            self.lower(p, "out", g, g * gw, (g + 1) * gw)

    @scoped
    def mix(self, p):
        s, r, q = self.s, self.r, self.tail
        base = self.part * s.count
        proj, fresh_ref = r["proj" + q], self.outs["fresh"]
        self.lowered = False

        def take(name):
            pieces = []
            for chunk in s.mix_chunks:
                for other, lo, _ in chunk:
                    if other == name:
                        pieces.append((lo, *s.place[name, lo]))
            return jnp.concatenate([proj[:, at : at + w] for _, at, w in sorted(pieces)], axis=1)

        values, writes, reads = take("value"), take("write"), take("read")
        at, _ = s.place["step", 0]
        steps = proj[:, at : at + LANES][:, : s.heads]
        step = jax.nn.softplus(steps + r["v_bias"][...])
        decay = jnp.exp(-step * jnp.exp(r["v_rate"][...]))
        head_row = lax.broadcasted_iota(jnp.int32, (s.heads, s.inner), 0)
        head_col = lax.broadcasted_iota(jnp.int32, (s.heads, s.inner), 1) // s.head
        widen = (head_row == head_col).astype(F32)
        exact = dict(preferred_element_type=F32, precision=lax.Precision.HIGHEST)
        step_wide = jnp.dot(step, widen, **exact)
        decay_wide = jnp.dot(decay, widen, **exact)
        r["decay" + q][...] = decay
        gw, st = s.group_width, s.state
        conv_w = r["v_cw"]
        taps = conv_w.shape[0]
        gates = take("gate")
        scaled_inputs, lone, activated = [], [], []
        for g in range(s.groups):
            fresh = jnp.concatenate(
                [values[:, g * gw : (g + 1) * gw], writes[:, g * st : (g + 1) * st], reads[:, g * st : (g + 1) * st]],
                axis=1,
            )
            fresh_ref[g, base : base + s.count, :] = fresh
            act = sigmoid_gate(r["conv" + q][g] + fresh * conv_w[taps - 1, g : g + 1, :])
            inputs, write, read = act[:, :gw], act[:, gw : gw + st], act[:, gw + st :]
            si = inputs * step_wide[:, g * gw : (g + 1) * gw]
            r["write" + q][g] = write
            r["vecs" + q][g] = read
            scaled_inputs.append(si)
            lone.append(jnp.sum(write * read, axis=1, keepdims=True))
        state = r["v_state"]
        per = s.heads // s.groups
        row = lax.broadcasted_iota(jnp.int32, (s.count, s.state), 0)
        self.need("state")

        def one(k, totals):
            found = []
            for g, total in enumerate(totals):
                held = state[base + k, g * per : (g + 1) * per].reshape(gw, st).astype(BF16)
                vec = jnp.where(row == k, r["vecs" + q][g], 0.0).astype(BF16)
                drawn = lax.dot_general(vec, held, (((1,), (1,)), ((), ())), preferred_element_type=F32)
                found.append(total + drawn)
            return tuple(found)

        drawn = lax.fori_loop(
            0, s.count, one, tuple(jnp.zeros((s.count, gw), F32) for _ in range(s.groups)), unroll=4
        )
        whole = [pl.ds(g * gw, gw) for g in range(s.groups)]
        for g in range(s.groups):
            cols = slice(g * gw, (g + 1) * gw)
            readout = decay_wide[:, cols] * drawn[g] + scaled_inputs[g] * lone[g]
            gated = readout * sigmoid_gate(gates[:, cols])
            mean = jnp.sum(gated * gated, axis=1, keepdims=True) / gw
            mixed = gated * lax.rsqrt(mean + norm_epsilon) * r["v_gg"][:, cols]
            r[p + "hid"][self.q, self.par, self.x, :, whole[g]] = mixed.astype(BF16)
            self.spread_start(p, g, DIRECT, whole[g])
        for g in range(s.groups):
            si = scaled_inputs[g]
            high = si.astype(BF16).astype(F32)
            fill = jnp.zeros((s.deep - 3 * s.count, gw), F32)
            r["left" + q][g] = jnp.concatenate([high, high, si - high, fill], axis=0).T.astype(BF16)

    @scoped
    def update(self, lo, hi):
        s, r = self.s, self.r
        q, first = self.tail, self.part * s.count
        state, left, gw, st = r["v_state"], r["left" + q], s.group_width, s.state
        per, block = s.heads // s.groups, 2
        row = lax.broadcasted_iota(jnp.int32, (s.count, st), 0)

        def one(j, carry):
            base = j * block
            for g in range(s.groups):
                write = r["write" + q][g]
                picked = jnp.concatenate([jnp.where(row == base + i, write, 0.0) for i in range(block)], axis=1)
                high = picked.astype(BF16).astype(F32)
                fill = jnp.zeros((s.deep - 3 * s.count, block * st), F32)
                right = jnp.concatenate([high, picked - high, high, fill], axis=0).astype(BF16)
                outer = jnp.dot(left[g], right, preferred_element_type=F32)
                for i in range(block):
                    decay = r["decay" + q][pl.ds(base + i, 1), :]
                    for h in range(g * per, (g + 1) * per):
                        at = (h - g * per) * s.head
                        new = outer[at : at + s.head, i * st : (i + 1) * st]
                        state[first + base + i, h] = state[first + base + i, h] * decay[:, h : h + 1] + new
            return carry

        lax.fori_loop(lo // block, hi // block, one, 0)

    @scoped
    def conv_past(self):
        s, r = self.s, self.r
        past, weight, conv = r["v_past"], r["v_cw"], r["conv" + self.tail]
        first = self.part * s.count
        taps = weight.shape[0]

        def one(k, carry):
            total = past[first + k, 0].astype(F32) * weight[0]
            for t in range(1, taps - 1):
                total = total + past[first + k, t].astype(F32) * weight[t]
            for g in range(s.groups):
                conv[g, pl.ds(k, 1), :] = total[g : g + 1, :]
            return carry

        lax.fori_loop(0, s.count, one, 0)


def step_kernel(s, plan, names, *refs):
    count = len(names)
    hbm = dict(zip(names, refs[:count]))
    outs = dict(zip(("next", "fresh", "state"), refs[count : count + 3]))
    r = dict(zip(plan.names, refs[count + 3 :]))
    r["v_state"] = outs["state"]
    sent = []
    bodies = [Body(s, r, part, sent) for part in range(s.parts)]
    body = bodies[0]
    order = [n for n in names if n not in ("stream", "gain1", "gain2", "gain3")]
    gains = r["gains"]
    width = s.depth // s.nt
    head = []
    if s.split:
        head.append(body.local(hbm["stream"], r["feat"], r["l0"].at[0]))
        head.append(body.local(hbm["gain1"], gains.at[0], r["l0"].at[1]))
    else:
        mine = pl.ds(pl.multiple_of(body.tp * width, LANES), width)
        head.append(body.local(hbm["stream"], r["feat"].at[:, :, :, mine], r["l0"].at[0]))
        for k in range(3):
            head.append(body.local(hbm["gain%d" % (k + 1)], gains.at[body.tp, pl.ds(k, 1)], r["l0"].at[k + 1]))
    sem = pltpu.get_barrier_semaphore()
    for d in range(1, s.n):
        pl.semaphore_signal(sem, inc=1, device_id={KV: lax.rem(body.me + d, s.n)}, device_id_type=MESH)
    for d in range(1, s.nt):
        pl.semaphore_signal(sem, inc=1, device_id={TP: lax.rem(body.tp + d, s.nt)}, device_id_type=MESH)
    for copy in head:
        copy.wait()
    first = {}
    for c in range(len(s.ff_chunks)):
        cols = body.columns(s.ff_chunks[c])
        for i, name in enumerate(("gate1", "up1")):
            first[c, i] = body.local(hbm[name].at[:, cols], r["v_" + name].at[:, cols], r["w1"].at[i, c])
    pl.semaphore_wait(sem, s.n + s.nt - 2)
    if not s.split:
        for d in range(1, s.nt):
            k = lax.rem(body.tp + d, s.nt)
            body.send(gains.at[body.tp], gains.at[body.tp], "n", tp=k)
        parts = sorted(range(s.parts), key=lambda part: part != ORDER[0] // 10000)
        for part in parts:
            block = r["feat"].at[:, part, :, mine]
            for d in range(1, s.nt):
                k = lax.rem(body.tp + d, s.nt)
                sent.append(copy_to(block, block, r["sent"].at[0], r["f"].at[part], tp=k))
                sent[-1].start()
        body.came(gains.at[pl.ds(0, s.nt - 1)], "n")

    def arrive(part):
        if not s.split:
            place = r["feat"].at[:, part, :, pl.ds(0, (s.nt - 1) * width)]
            pltpu.make_async_copy(place, place, r["f"].at[part]).wait()
        rows = r["feat"][:, part].astype(F32)
        r["b" + str(part)][...] = rows.reshape(s.rows, s.depth).astype(BF16)

    rest = {}
    begun = set()

    def ready(c):
        if c in begun:
            return
        first[c, 0].wait()
        first[c, 1].wait()
        if not begun:
            for i, name in enumerate(order):
                if name not in ("gate1", "up1"):
                    rest[name] = body.local(hbm[name], r["v_" + name], r["w"].at[i])
        begun.add(c)

    waited = set()

    def need(*wanted):
        for name in wanted:
            if name not in waited:
                waited.add(name)
                rest[name].wait()

    for body in bodies:
        body.need, body.ready, body.outs, body.arrive = need, ready, outs, arrive
    for code in ORDER:
        bodies[code // 10000].event(code // 1000 % 10, code // 10 % 100, code % 10)
    for copy in sent:
        copy.wait_send()


def write_kernel(s, blocks, past_ref, fresh_ref, next_ref, state_ref, state_out, past_out, next_out, moved, sem):
    taps, count = past_ref.shape[1], past_ref.shape[0]
    step = count // blocks
    copies = [pltpu.make_async_copy(next_ref, next_out, sem.at[blocks])]
    for k in range(blocks):
        rows = pl.ds(k * step, step)
        copies.append(pltpu.make_async_copy(state_ref.at[rows], state_out.at[rows], sem.at[k]))
    for copy in copies:
        copy.start()

    def one(k, carry):
        for t in range(taps - 1):
            moved[k, t] = past_ref[k, t + 1]
        newest = [fresh_ref[g, pl.ds(k, 1), :] for g in range(s.groups)]
        moved[k, taps - 1] = jnp.concatenate(newest, axis=0).astype(BF16)
        return carry

    lax.fori_loop(0, count, one, 0)
    copies.append(pltpu.make_async_copy(moved, past_out, sem.at[blocks + 1]))
    copies[-1].start()
    for copy in copies:
        copy.wait()


def gathered(stream, gains):
    n = lax.axis_size(TP)
    features = lax.all_gather(stream, TP, axis=1, tiled=True)
    packed = lax.all_gather(jnp.stack(gains), TP, axis=1, tiled=True)
    return features, packed


def on_device(
    stream,
    ssm_state,
    conv_state,
    first_gain,
    first_gate,
    first_up,
    first_down,
    mix_gain,
    gate_in,
    value_in,
    write_in,
    read_in,
    step_in,
    conv_weight,
    step_bias,
    log_decay_rate,
    group_gain,
    out_weight,
    last_norm_gain,
    second_gate,
    second_up,
    second_down,
):
    n, nt = lax.axis_size(KV), lax.axis_size(TP)
    rows, width = stream.shape
    depth, units = first_gate.shape
    heads, head, state = ssm_state.shape[1:]
    groups = conv_weight.shape[1]
    split = width % LANES != 0
    s = Sizes(n, nt, rows, depth, units, heads, head, state, groups, split)
    if split:
        features, packed = gathered(stream, [first_gain, mix_gain, last_norm_gain])
        named = {"stream": features.reshape(n, s.parts, s.count, depth), "gain1": packed}
    else:
        named = {
            "stream": stream.reshape(n, s.parts, s.count, width),
            "gain1": first_gain[None],
            "gain2": mix_gain[None],
            "gain3": last_norm_gain[None],
        }
    weights = {
        "gate1": first_gate,
        "up1": first_up,
        "down1": first_down,
        "value": value_in,
        "gate": gate_in,
        "write": write_in,
        "read": read_in,
        "step": step_in.T,
        "cw": conv_weight,
        "bias": step_bias[None],
        "rate": log_decay_rate[None],
        "gg": group_gain[None],
        "past": conv_state,
        "state": ssm_state,
        "out": out_weight,
        "gate2": second_gate,
        "up2": second_up,
        "down2": second_down,
    }
    plan = make_plan(s, [(k, v.shape, v.dtype) for k, v in weights.items()])
    named.update(weights)
    result, fresh, held = pl.pallas_call(
        functools.partial(step_kernel, s, plan, list(named)),
        out_shape=[
            pltpu.VMEM((n, s.parts, s.count, depth if split else width), BF16),
            pltpu.VMEM((groups, rows // n, s.channels), F32),
            pltpu.VMEM(ssm_state.shape, ssm_state.dtype),
        ],
        in_specs=[HB] * len(named),
        out_specs=[VM] * 3,
        scratch_shapes=plan.shapes,
        compiler_params=pltpu.CompilerParams(
            collective_id=0, has_side_effects=True, vmem_limit_bytes=48 * 1024 * 1024
        ),
    )(*named.values())
    if split:
        me = lax.axis_index(TP)
        result = lax.dynamic_slice_in_dim(result, me * width, width, axis=3)
    blocks = 8
    state_next, past_next, stream_next = pl.pallas_call(
        functools.partial(write_kernel, s, blocks),
        out_shape=[
            jax.ShapeDtypeStruct(ssm_state.shape, ssm_state.dtype),
            jax.ShapeDtypeStruct(conv_state.shape, conv_state.dtype),
            jax.ShapeDtypeStruct(result.shape, BF16),
        ],
        in_specs=[VM] * 4,
        out_specs=[HB] * 3,
        scratch_shapes=[pltpu.VMEM(conv_state.shape, BF16), pltpu.SemaphoreType.DMA((blocks + 2,))],
        compiler_params=pltpu.CompilerParams(vmem_limit_bytes=8 * 1024 * 1024),
    )(conv_state, fresh, result, held)
    return (stream_next.reshape(stream.shape), state_next, past_next)


def solution(mesh):
    return jax.shard_map(
        on_device,
        mesh=mesh,
        in_specs=(
            P(None, (KV, TP)),
            P(KV, TP, None, None),
            P(KV, None, TP, None),
            P((KV, TP)),
            P(KV, TP),
            P(KV, TP),
            P(TP, KV),
            P((KV, TP)),
            P(KV, TP),
            P(KV, TP),
            P(KV, TP),
            P(KV, TP),
            P(KV, TP),
            P(None, TP, None),
            P(TP),
            P(TP),
            P(TP),
            P(TP, KV),
            P((KV, TP)),
            P(KV, TP),
            P(KV, TP),
            P(TP, KV),
        ),
        out_specs=(P(None, (KV, TP)), P(KV, TP, None, None), P(KV, None, TP, None)),
        check_vma=False,
    )
```

```python
import functools

import jax
import jax.numpy as jnp
from jax import lax
from jax.experimental import pallas as pl
from jax.experimental.pallas import tpu as pltpu
from jax.sharding import PartitionSpec as P

norm_epsilon = 1e-06
MESH = pl.DeviceIdType.MESH
LANES = 128
KV, TP = "kv", "tp"
DIRECT, THREE, FIRST = "d", "t", "f"
VM = pl.BlockSpec(memory_space=pltpu.VMEM)
HB = pl.BlockSpec(memory_space=pltpu.HBM)
F32 = jnp.float32
BF16 = jnp.bfloat16


def sigmoid_gate(v):
    return v / (1.0 + jnp.exp(-v))


def copy_to(src, dst, send, recv, **where):
    return pltpu.make_async_remote_copy(
        src_ref=src, dst_ref=dst, send_sem=send, recv_sem=recv, device_id=where, device_id_type=MESH
    )


def tag(p, stage, c):
    return p + stage + str(c)


class Plan:
    def __init__(self):
        self.names, self.shapes = [], []

    def add(self, name, shape, dtype):
        self.names.append(name)
        self.shapes.append(pltpu.VMEM(shape, dtype))

    def sem(self, name, *shape):
        if "1" + name[1:] in self.names and name[0] == "2":
            return
        self.names.append(name)
        self.shapes.append(pltpu.SemaphoreType.DMA(shape or (1,)))


def cut(total, shares):
    ends = [0] + [max(1, round(total * s)) for s in shares] + [total]
    return [(a, b) for a, b in zip(ends, ends[1:]) if b > a]


SUM = {DIRECT: "xz", THREE: "xpc", FIRST: "pxc"}
SPREAD = {DIRECT: "hg", THREE: "ijg", FIRST: "ijk"}
FF_CHUNKS = [(DIRECT, THREE, 4), (FIRST, FIRST, 6), (THREE, DIRECT, 6), (THREE, DIRECT, 6)]
MIX_WAYS = (DIRECT, FIRST, DIRECT, DIRECT)
PARTS, UPDATE, UPDATES = 2, 8, 4
ORDER = [
    0, 10, 20, 30, 1, 11, 10010, 10000, 21, 10020, 2, 31, 12, 10030,
    22, 10011, 10001, 32, 10021, 3, 13, 23, 10002, 10031, 10012, 33, 4, 10022,
    14, 10032, 24, 10003, 5, 10013, 15, 34, 10023, 10004, 25, 10033, 10014, 16,
    35, 1000, 10024, 10034, 10015, 1001, 10005, 10025, 1002, 10035, 10016, 11000, 2000, 2020,
    2010, 2030, 11001, 2001, 2011, 2021, 11002, 12010, 12000, 12020, 2031, 2012, 12011, 2002,
    2022, 12030, 12021, 12001, 2032, 2013, 3000, 12031, 8030, 8010, 8000, 12012, 4001, 12022,
    4011, 12002, 12013, 12032, 13000, 4002, 4012, 5000, 14001, 18000, 14011, 5001, 5002, 6000,
    6020, 14002, 6010, 14012, 15000, 6030, 6001, 15001, 6021, 6011, 15002, 16010, 16000, 16020,
    8020, 16030, 6002, 6031, 6012, 6022, 16001, 6003, 6032, 16011, 16021, 18010, 18020, 18030,
    6023, 6013, 16002, 16031, 16012, 6004, 6033, 16022, 6014, 16032, 16003, 6024, 16013, 16023,
    16004, 16033, 16014, 6034, 6005, 16024, 6015, 16015, 16034, 6025, 16005, 16025, 6016, 6035,
    7000, 16016, 16035, 17000, 7001, 17001,
]


class Sizes:
    def __init__(self, n, nt, rows, depth, units, heads, head, state, groups, split):
        self.n, self.nt, self.rows, self.depth, self.units = n, nt, rows, depth, units
        self.heads, self.head, self.state, self.groups, self.split = heads, head, state, groups, split
        self.zn, self.zh, self.ny = n // 2, n // 4, nt // 2
        self.parts = PARTS
        self.all_rows, self.rows = rows, rows // PARTS
        self.count = self.rows // n
        self.deep = -(-3 * self.count // LANES) * LANES
        tiles = units // LANES
        shares = [share for _, _, share in FF_CHUNKS]
        ends = [sum(shares[: i + 1]) / sum(shares) for i in range(len(shares) - 1)]
        self.ff_chunks = [
            (out, back, a * LANES, z * LANES) for (out, back, _), (a, z) in zip(FF_CHUNKS, cut(tiles, ends))
        ]
        self.inner = heads * head
        self.group_width = self.inner // groups
        self.channels = self.group_width + 2 * state
        v = self.inner // LANES
        vec = groups * state
        gb = max(1, v * 5 // 8)
        self.mix_chunks = [
            [("value", 0, v // 2 * LANES)],
            [("gate", 0, gb * LANES)],
            [("value", v // 2 * LANES, v * LANES), ("write", 0, vec)],
            [("read", 0, vec), ("step", 0, LANES), ("gate", gb * LANES, v * LANES)],
        ]
        spans, at = [], 0
        self.place = {}
        for chunk in self.mix_chunks:
            lo = at
            for name, a, z in chunk:
                self.place[name, a] = (at, z - a)
                at += z - a
            spans.append((lo, at))
        self.mix_spans = [(way, None, a, z) for way, (a, z) in zip(MIX_WAYS, spans)]
        self.mix_width = at


def add_sum(plan, s, p, width, chunks):
    zn, zh, cnt, n = s.zn, s.zh, s.count, s.n
    zl = max(1, zh - 1)
    plan.add(p + "part", (zh, 2, 2, cnt, width), BF16)
    plan.add(p + "near", (zh, 2, cnt, width), BF16)
    plan.add(p + "mid", (zh, 2, cnt, width), BF16)
    plan.add(p + "far", (zn - 1, cnt, width), BF16)
    plan.add(p + "near2", (zh, cnt, width), BF16)
    plan.add(p + "mid2", (zh, cnt, width), BF16)
    plan.add(p + "far2", (zl, cnt, width), BF16)
    plan.add(p + "side", (n, s.count, LANES), F32)
    plan.add(p + "sides", (n - 1, s.count, LANES), F32)
    plan.sem(p + "e")
    for c, chunk in enumerate(chunks):
        for stage in SUM[chunk[0]]:
            plan.sem(p + stage + str(c))


def add_spread(plan, s, p, width, chunks):
    plan.add(p + "hid", (s.zh, 2, 2, s.count, width), BF16)
    for c, chunk in enumerate(chunks):
        for stage in SPREAD[chunk[1]]:
            plan.sem(p + stage + str(c))


def add_finish(plan, s, p, last):
    plan.add(p + "acc", (s.rows, s.depth), F32)
    if last and not s.split:
        plan.add(p + "t0", (s.nt, s.rows, s.depth // s.nt), BF16)
        plan.add(p + "t1", (s.nt - 1, s.rows, s.depth // s.nt), BF16)
        plan.sem(p + "t")
        return
    for name in ("t0", "t1", "t2", "feat"):
        plan.add(p + name, (s.rows, s.depth), BF16)
    plan.add(p + "t3", (max(1, s.ny - 1), s.rows, s.depth), BF16)
    for stage in "uv":
        plan.sem(p + stage)


def make_plan(s, weights):
    plan = Plan()
    for name, shape, dtype in weights:
        if name != "state":
            plan.add("v_" + name, shape, dtype)
    plan.sem("w", len(weights))
    plan.sem("w1", 2, len(s.ff_chunks))
    plan.add("feat", (s.n, s.parts, s.count, s.depth), BF16)
    plan.add("gains", (s.nt, 3, s.depth // s.nt) if not s.split else (1, 3, s.depth), F32)
    plan.sem("l0", 4)
    plan.sem("sent")
    plan.sem("f", s.parts)
    plan.sem("n")
    for part in range(s.parts):
        q = str(part)
        plan.add("b" + q, (s.rows, s.depth), BF16)
        for p in ("1" + q, "2" + q):
            add_sum(plan, s, p, 2 * s.units, s.ff_chunks)
            add_spread(plan, s, p, s.units, s.ff_chunks)
        add_sum(plan, s, "m" + q, s.mix_width, s.mix_spans)
        add_spread(plan, s, "m" + q, s.inner, [(DIRECT, DIRECT)] * s.groups)
        add_finish(plan, s, "1" + q, False)
        add_finish(plan, s, "m" + q, False)
        add_finish(plan, s, "2" + q, True)
        plan.add("proj" + q, (s.count, s.mix_width), F32)
        plan.add("conv" + q, (s.groups, s.count, s.channels), F32)
        plan.add("vecs" + q, (s.groups, s.count, s.state), F32)
        plan.add("left" + q, (s.groups, s.group_width, s.deep), BF16)
        plan.add("write" + q, (s.groups, s.count, s.state), F32)
        plan.add("decay" + q, (s.count, s.heads), F32)
    return plan


def scoped(f):
    @functools.wraps(f)
    def inner(*args):
        tag = "_".join(str(a) for a in args if isinstance(a, (str, int)))
        with jax.named_scope(f.__name__ + "_" + tag):
            return f(*args)

    return inner


class Body:
    def __init__(self, s, r, part, sent):
        self.s, self.r, self.sent, self.part, self.tail = s, r, sent, part, str(part)
        self.stage = None
        me = lax.axis_index(KV)
        self.me, self.z, self.x = me, me // 2, lax.rem(me, 2)
        self.q, self.par = me // 4, lax.rem(me // 2, 2)
        self.tp = lax.axis_index(TP)
        self.y, self.core = self.tp // 2, lax.rem(self.tp, 2)
        self.xpeer = self.z * 2 + 1 - self.x
        self.ppeer = (self.q * 2 + 1 - self.par) * 2 + self.x

    def start(self, copy):
        copy.start()
        self.sent.append(copy)
        return copy

    def sem(self, name):
        return self.r[name if name in self.r else "1" + name[1:]].at[0]

    def send(self, src, dst, sem, **where):
        return self.start(copy_to(src, dst, self.r["sent"].at[0], self.sem(sem), **where))

    def came(self, place, sem):
        pltpu.make_async_copy(place, place, self.sem(sem)).wait()

    def local(self, src, dst, sem):
        copy = pltpu.make_async_copy(src, dst, sem)
        copy.start()
        return copy

    @scoped
    def side_send(self, p):
        side, sides = self.r[p + "side"], self.r[p + "sides"]
        for d in range(1, self.s.n):
            k = lax.rem(self.me + d, self.s.n)
            self.send(side.at[k], sides.at[d - 1], p + "e", kv=k)

    @scoped
    def row_factor(self, p):
        s = self.s
        total = self.r[p + "side"][self.me]
        self.came(self.r[p + "sides"], p + "e")
        for d in range(s.n - 1):
            total = total + self.r[p + "sides"][d]
        return lax.rsqrt(total / (s.depth * s.n) + norm_epsilon)[:, :1]

    def columns(self, chunk, scale=1):
        return pl.ds(chunk[2] * scale, (chunk[3] - chunk[2]) * scale)

    def across(self, q):
        return (q * 2 + self.par) * 2 + self.x

    def sum_start(self, p, c, kind, cols):
        part, near = self.r[p + "part"], self.r[p + "near"].at[:, :, :, cols]
        if kind == FIRST:
            self.send(part.at[:, 1 - self.par, :, :, cols], near, tag(p, "p", c), kv=self.ppeer)
        else:
            self.send(part.at[:, :, 1 - self.x, :, cols], near, tag(p, "x", c), kv=self.xpeer)

    @scoped
    def sum_step(self, p, name, c, kind, cols):
        r, s = self.r, self.s
        part, near, mid = r[p + "part"], r[p + "near"], r[p + "mid"]
        near2, mid2 = r[p + "near2"], r[p + "mid2"]
        sem = tag(p, name, c)
        if name == "c":
            kept = mid[:, self.x, :, cols] if kind == FIRST else mid[:, self.par, :, cols]
            self.came(near2.at[:, :, cols], tag(p, "x" if kind == FIRST else "p", c))
            mid2[:, :, cols] = (kept.astype(F32) + near2[:, :, cols].astype(F32)).astype(BF16)
            for d in range(1, s.zh):
                q = lax.rem(self.q + d, s.zh)
                self.send(mid2.at[q, :, cols], r[p + "far2"].at[d - 1, :, cols], sem, kv=self.across(q))
            return
        self.came(near.at[:, :, :, cols], tag(p, "p" if kind == FIRST else "x", c))
        kept = part[:, self.par, :, :, cols] if kind == FIRST else part[:, :, self.x, :, cols]
        mid[:, :, :, cols] = (kept.astype(F32) + near[:, :, :, cols].astype(F32)).astype(BF16)
        if name == "z":
            for d in range(1, s.zn):
                z = lax.rem(self.z + d, s.zn)
                src = mid.at[z // 2, lax.rem(z, 2), :, cols]
                self.send(src, r[p + "far"].at[d - 1, :, cols], sem, kv=z * 2 + self.x)
        elif name == "p":
            self.send(mid.at[:, 1 - self.par, :, cols], near2.at[:, :, cols], sem, kv=self.ppeer)
        else:
            self.send(mid.at[:, 1 - self.x, :, cols], near2.at[:, :, cols], sem, kv=self.xpeer)

    @scoped
    def sum_total(self, p, c, kind, cols):
        r = self.r
        if kind == DIRECT:
            own, far, sem = r[p + "mid"].at[self.q, self.par], r[p + "far"], tag(p, "z", c)
        else:
            own, far, sem = r[p + "mid2"].at[self.q], r[p + "far2"], tag(p, "c", c)
        total = own[:, cols].astype(F32)
        self.came(far.at[:, :, cols], sem)
        for d in range(far.shape[0]):
            total = total + far[d, :, cols].astype(F32)
        return total

    def spot(self, p, z, cols):
        return self.r[p + "hid"].at[z // 2, lax.rem(z, 2), self.x, :, cols]

    def spread_start(self, p, c, kind, cols):
        s = self.s
        mine = self.spot(p, self.z, cols)
        if kind == DIRECT:
            for d in range(1, s.zn):
                z = lax.rem(self.z + d, s.zn)
                self.send(mine, mine, tag(p, "h", c), kv=z * 2 + self.x)
        else:
            for d in range(1, s.zh):
                self.send(mine, mine, tag(p, "i", c), kv=self.across(lax.rem(self.q + d, s.zh)))

    @scoped
    def spread_step(self, p, name, c, kind, cols):
        r = self.r
        hid = r[p + "hid"]
        first = kind == FIRST
        if name == "g" and kind == DIRECT:
            self.came(r[p + "far"].at[:, :, cols], tag(p, "h", c))
        elif name == "j":
            self.came(r[p + "far2"].at[:, :, cols], tag(p, "i", c))
        elif name == "g":
            self.came(hid.at[:, 1 - self.par, self.x, :, cols], tag(p, "j", c))
        else:
            self.came(hid.at[:, self.par, 1 - self.x, :, cols], tag(p, "j", c))
        if name == "j":
            own = hid.at[:, self.par, self.x, :, cols]
            self.send(own, own, tag(p, "j", c), kv=self.xpeer if first else self.ppeer)
        elif name == "g":
            own = hid.at[:, :, self.x, :, cols]
            self.send(own, own, tag(p, "g", c), kv=self.xpeer)
        else:
            own = hid.at[:, self.par, :, :, cols]
            self.send(own, own, tag(p, "k", c), kv=self.ppeer)

    @scoped
    def spread_end(self, p, c, kind, cols):
        hid = self.r[p + "hid"]
        if kind == FIRST:
            self.came(hid.at[:, 1 - self.par, :, :, cols], tag(p, "k", c))
        else:
            self.came(hid.at[:, :, 1 - self.x, :, cols], tag(p, "g", c))
        self.need("out" if p[0] == "m" else "down" + p[0])

    @scoped
    def finish(self, p, weight, before, k):
        r, s = self.r, self.s
        t0, t1, t2, t3, feat = (r[p + name] for name in ("t0", "t1", "t2", "t3", "feat"))
        if k == 0:
            t0[...] = r[p + "acc"][...].astype(BF16)
            for d in range(1, s.ny):
                yp = lax.rem(self.y + d, s.ny)
                self.send(t0, t3.at[d - 1], p + "u", tp=yp * 2 + self.core)
        elif k == 1:
            total = t0[...].astype(F32)
            self.came(t3, p + "u")
            for d in range(s.ny - 1):
                total = total + t3[d].astype(F32)
            t2[...] = total.astype(BF16)
            self.send(t2, t1, p + "v", tp=self.tp + 1 - 2 * self.core)
        else:
            self.came(t1, p + "v")
            total = t2[...].astype(F32) + t1[...].astype(F32)
            feat[...] = (before[...].astype(F32) + weight * total).astype(BF16)

    @scoped
    def last_start(self, p):
        r, s = self.r, self.s
        width = s.depth // s.nt
        t0, t1 = r[p + "t0"], r[p + "t1"]
        for k in range(s.nt):
            t0[k] = r[p + "acc"][:, k * width : (k + 1) * width].astype(BF16)
        for d in range(1, s.nt):
            k = lax.rem(self.tp + d, s.nt)
            self.send(t0.at[k], t1.at[d - 1], p + "t", tp=k)

    @scoped
    def last_end(self, p, weight, before, out_ref):
        r, s = self.r, self.s
        width = s.depth // s.nt
        t1 = r[p + "t1"]
        total = r[p + "t0"][self.tp].astype(F32)
        self.came(t1, p + "t")
        for d in range(s.nt - 1):
            total = total + t1[d].astype(F32)
        cols = pl.ds(pl.multiple_of(self.tp * width, LANES), width)
        mine = before[:, cols].astype(F32)
        out_ref[:, self.part] = (mine + weight * total).reshape(s.n, s.count, width).astype(BF16)

    def finish_last(self, p, weight, before, out_ref, k):
        s = self.s
        if s.split:
            for j in ((0,), (1, 2))[k]:
                self.finish(p, weight, before, j)
            if k == 1:
                feat = self.r[p + "feat"][...].astype(F32)
                out_ref[:, self.part] = feat.reshape(s.n, s.count, s.depth).astype(BF16)
        elif k == 0:
            self.last_start(p)
        else:
            self.last_end(p, weight, before, out_ref)

    def gain(self, k):
        gains = self.r["gains"]
        return jnp.concatenate([gains[t, k : k + 1, :] for t in range(gains.shape[0])], axis=1)

    @scoped
    def normed(self, p, feat, k):
        s = self.s
        values = feat[...].astype(F32)
        squares = jnp.sum(values * values, axis=1, keepdims=True)
        self.r[p + "side"][...] = jnp.broadcast_to(squares, (s.rows, LANES)).reshape(s.n, s.count, LANES)
        return (values * self.gain(k)).astype(BF16)

    def put_part(self, p, lo, value):
        s = self.s
        w = value.shape[1]
        self.r[p + "part"][:, :, :, :, pl.ds(lo, w)] = value.reshape(s.zh, 2, 2, s.count, w).astype(BF16)

    def event(self, stage, c, k):
        s, r, q = self.s, self.r, self.tail
        before = (r["b" + q], r["1" + q + "feat"], r["m" + q + "feat"])
        if stage == UPDATE:
            self.update(c * s.count // UPDATES, (c + 1) * s.count // UPDATES)
        elif stage in (0, 6):
            self.feed_forward(("1" if stage == 0 else "2") + q, before[stage // 3], stage // 3, c, k)
        elif stage == 1:
            self.finish("1" + q, 0.5, before[0], k)
        elif stage == 2:
            self.project("m" + q, before[1], c, k)
        elif stage == 3:
            self.mix("m" + q)
        elif stage == 4 and c < s.groups:
            self.mixed("m" + q, c, k)
        elif stage == 5:
            self.finish("m" + q, 1.0, before[1], k)
        elif stage == 7:
            self.finish_last("2" + q, 0.5, before[2], self.outs["next"], k)

    def begin(self, p, feat, k):
        if self.stage is None:
            self.arrive(self.part)
        if self.stage != p:
            self.scaled, self.factor, self.lowered = self.normed(p, feat, k), None, False
            self.stage, self.started = p, 0
        self.started += 1

    @scoped
    def multiply(self, p, c):
        r = self.r
        if p[0] == "1":
            self.ready(c)
        else:
            self.need("gate2", "up2")
        _, _, lo, hi = self.s.ff_chunks[c]
        for i, w in enumerate(("gate", "up")):
            weight = r["v_" + w + p[0]]
            self.put_part(p, 2 * lo + i * (hi - lo), jnp.dot(self.scaled, weight[:, lo:hi], preferred_element_type=F32))

    def activated(self, p, c, way, cols):
        total = self.sum_total(p, c, way, cols)
        if self.factor is None:
            self.factor = self.row_factor(p)
        return total * self.factor

    @scoped
    def lower(self, p, name, c, lo, hi):
        s, r = self.s, self.r
        hidden = r[p + "hid"][:, :, :, :, pl.ds(lo, hi - lo)].astype(F32).reshape(s.rows, hi - lo)
        weight = r["v_" + name]
        value = jnp.dot(hidden.astype(BF16), weight[lo:hi, :], preferred_element_type=F32)
        if not self.lowered:
            r[p + "acc"][...] = value
        else:
            r[p + "acc"][...] += value
        self.lowered = True

    def feed_forward(self, p, feat, gain, c, k):
        chunk = self.s.ff_chunks[c]
        way, back, lo, hi = chunk
        there, home = SUM[way], SPREAD[back]
        cols, wide = self.columns(chunk), self.columns(chunk, 2)
        at = k - len(there)
        if k == 0:
            self.begin(p, feat, gain)
            self.multiply(p, c)
            self.sum_start(p, c, way, wide)
            if self.started == 2:
                self.side_send(p)
        elif at < 0:
            self.sum_step(p, there[k], c, way, wide)
        elif at == 0:
            total = self.activated(p, c, way, wide)
            hidden = sigmoid_gate(total[:, : hi - lo]) * total[:, hi - lo :]
            self.r[p + "hid"][self.q, self.par, self.x, :, cols] = hidden.astype(BF16)
            self.spread_start(p, c, back, cols)
        elif at < len(home):
            self.spread_step(p, home[at], c, back, cols)
        else:
            self.spread_end(p, c, back, cols)
            self.lower(p, "down" + p[0], c, lo, hi)

    @scoped
    def multiply_mixer(self, p, c):
        s, r = self.s, self.r
        for name, lo, hi in s.mix_chunks[c]:
            at, w = s.place[name, lo]
            weight = r["v_" + name]
            if name == "step":
                value = lax.dot_general(
                    self.scaled, weight[...], (((1,), (1,)), ((), ())), preferred_element_type=F32
                )
                self.put_part(p, at, jnp.zeros((s.rows, LANES), F32))
                self.put_part(p, at, value)
            else:
                self.put_part(p, at, jnp.dot(self.scaled, weight[:, lo:hi], preferred_element_type=F32))

    def project(self, p, feat, c, k):
        s, r = self.s, self.r
        chunk = s.mix_spans[c]
        way, _, lo, hi = chunk
        cols = self.columns(chunk)
        if k == 0:
            self.need("value", "write", "read", "step", "gate", "bias", "rate", "cw", "gg", "past")
            self.begin(p, feat, 1)
            self.multiply_mixer(p, c)
            self.sum_start(p, c, way, cols)
            if self.started == 2:
                self.side_send(p)
            if c == 2:
                self.conv_past()
        elif k < len(SUM[way]):
            self.sum_step(p, SUM[way][k], c, way, cols)
        else:
            r["proj" + self.tail][:, lo:hi] = self.activated(p, c, way, cols).astype(BF16).astype(F32)

    def mixed(self, p, g, k):
        gw = self.s.group_width
        cols = pl.ds(g * gw, gw)
        if k == 1:
            self.spread_step(p, "g", g, DIRECT, cols)
        else:
            self.spread_end(p, g, DIRECT, cols)
            self.lower(p, "out", g, g * gw, (g + 1) * gw)

    @scoped
    def mix(self, p):
        s, r, q = self.s, self.r, self.tail
        base = self.part * s.count
        proj, fresh_ref = r["proj" + q], self.outs["fresh"]
        self.lowered = False

        def take(name):
            pieces = []
            for chunk in s.mix_chunks:
                for other, lo, _ in chunk:
                    if other == name:
                        pieces.append((lo, *s.place[name, lo]))
            return jnp.concatenate([proj[:, at : at + w] for _, at, w in sorted(pieces)], axis=1)

        values, writes, reads = take("value"), take("write"), take("read")
        at, _ = s.place["step", 0]
        steps = proj[:, at : at + LANES][:, : s.heads]
        step = jax.nn.softplus(steps + r["v_bias"][...])
        decay = jnp.exp(-step * jnp.exp(r["v_rate"][...]))
        head_row = lax.broadcasted_iota(jnp.int32, (s.heads, s.inner), 0)
        head_col = lax.broadcasted_iota(jnp.int32, (s.heads, s.inner), 1) // s.head
        widen = (head_row == head_col).astype(F32)
        exact = dict(preferred_element_type=F32, precision=lax.Precision.HIGHEST)
        step_wide = jnp.dot(step, widen, **exact)
        decay_wide = jnp.dot(decay, widen, **exact)
        r["decay" + q][...] = decay
        gw, st = s.group_width, s.state
        conv_w = r["v_cw"]
        taps = conv_w.shape[0]
        gates = take("gate")
        scaled_inputs, lone, activated = [], [], []
        for g in range(s.groups):
            fresh = jnp.concatenate(
                [values[:, g * gw : (g + 1) * gw], writes[:, g * st : (g + 1) * st], reads[:, g * st : (g + 1) * st]],
                axis=1,
            )
            fresh_ref[g, base : base + s.count, :] = fresh
            act = sigmoid_gate(r["conv" + q][g] + fresh * conv_w[taps - 1, g : g + 1, :])
            inputs, write, read = act[:, :gw], act[:, gw : gw + st], act[:, gw + st :]
            si = inputs * step_wide[:, g * gw : (g + 1) * gw]
            r["write" + q][g] = write
            r["vecs" + q][g] = read
            scaled_inputs.append(si)
            lone.append(jnp.sum(write * read, axis=1, keepdims=True))
        state = r["v_state"]
        per = s.heads // s.groups
        row = lax.broadcasted_iota(jnp.int32, (s.count, s.state), 0)
        self.need("state")

        def one(k, totals):
            found = []
            for g, total in enumerate(totals):
                held = state[base + k, g * per : (g + 1) * per].reshape(gw, st).astype(BF16)
                vec = jnp.where(row == k, r["vecs" + q][g], 0.0).astype(BF16)
                drawn = lax.dot_general(vec, held, (((1,), (1,)), ((), ())), preferred_element_type=F32)
                found.append(total + drawn)
            return tuple(found)

        drawn = lax.fori_loop(
            0, s.count, one, tuple(jnp.zeros((s.count, gw), F32) for _ in range(s.groups)), unroll=4
        )
        whole = [pl.ds(g * gw, gw) for g in range(s.groups)]
        for g in range(s.groups):
            cols = slice(g * gw, (g + 1) * gw)
            readout = decay_wide[:, cols] * drawn[g] + scaled_inputs[g] * lone[g]
            gated = readout * sigmoid_gate(gates[:, cols])
            mean = jnp.sum(gated * gated, axis=1, keepdims=True) / gw
            mixed = gated * lax.rsqrt(mean + norm_epsilon) * r["v_gg"][:, cols]
            r[p + "hid"][self.q, self.par, self.x, :, whole[g]] = mixed.astype(BF16)
            self.spread_start(p, g, DIRECT, whole[g])
        for g in range(s.groups):
            si = scaled_inputs[g]
            high = si.astype(BF16).astype(F32)
            fill = jnp.zeros((s.deep - 3 * s.count, gw), F32)
            r["left" + q][g] = jnp.concatenate([high, high, si - high, fill], axis=0).T.astype(BF16)

    @scoped
    def update(self, lo, hi):
        s, r = self.s, self.r
        q, first = self.tail, self.part * s.count
        state, left, gw, st = r["v_state"], r["left" + q], s.group_width, s.state
        per, block = s.heads // s.groups, 2
        row = lax.broadcasted_iota(jnp.int32, (s.count, st), 0)

        def one(j, carry):
            base = j * block
            for g in range(s.groups):
                write = r["write" + q][g]
                picked = jnp.concatenate([jnp.where(row == base + i, write, 0.0) for i in range(block)], axis=1)
                high = picked.astype(BF16).astype(F32)
                fill = jnp.zeros((s.deep - 3 * s.count, block * st), F32)
                right = jnp.concatenate([high, picked - high, high, fill], axis=0).astype(BF16)
                outer = jnp.dot(left[g], right, preferred_element_type=F32)
                for i in range(block):
                    decay = r["decay" + q][pl.ds(base + i, 1), :]
                    for h in range(g * per, (g + 1) * per):
                        at = (h - g * per) * s.head
                        new = outer[at : at + s.head, i * st : (i + 1) * st]
                        state[first + base + i, h] = state[first + base + i, h] * decay[:, h : h + 1] + new
            return carry

        lax.fori_loop(lo // block, hi // block, one, 0)

    @scoped
    def conv_past(self):
        s, r = self.s, self.r
        past, weight, conv = r["v_past"], r["v_cw"], r["conv" + self.tail]
        first = self.part * s.count
        taps = weight.shape[0]

        def one(k, carry):
            total = past[first + k, 0].astype(F32) * weight[0]
            for t in range(1, taps - 1):
                total = total + past[first + k, t].astype(F32) * weight[t]
            for g in range(s.groups):
                conv[g, pl.ds(k, 1), :] = total[g : g + 1, :]
            return carry

        lax.fori_loop(0, s.count, one, 0)


def step_kernel(s, plan, names, *refs):
    count = len(names)
    hbm = dict(zip(names, refs[:count]))
    outs = dict(zip(("next", "fresh", "state"), refs[count : count + 3]))
    r = dict(zip(plan.names, refs[count + 3 :]))
    r["v_state"] = outs["state"]
    sent = []
    bodies = [Body(s, r, part, sent) for part in range(s.parts)]
    body = bodies[0]
    order = [n for n in names if n not in ("stream", "gain1", "gain2", "gain3")]
    gains = r["gains"]
    width = s.depth // s.nt
    head = []
    if s.split:
        head.append(body.local(hbm["stream"], r["feat"], r["l0"].at[0]))
        head.append(body.local(hbm["gain1"], gains.at[0], r["l0"].at[1]))
    else:
        mine = pl.ds(pl.multiple_of(body.tp * width, LANES), width)
        head.append(body.local(hbm["stream"], r["feat"].at[:, :, :, mine], r["l0"].at[0]))
        for k in range(3):
            head.append(body.local(hbm["gain%d" % (k + 1)], gains.at[body.tp, pl.ds(k, 1)], r["l0"].at[k + 1]))
    sem = pltpu.get_barrier_semaphore()
    for d in range(1, s.n):
        pl.semaphore_signal(sem, inc=1, device_id={KV: lax.rem(body.me + d, s.n)}, device_id_type=MESH)
    for d in range(1, s.nt):
        pl.semaphore_signal(sem, inc=1, device_id={TP: lax.rem(body.tp + d, s.nt)}, device_id_type=MESH)
    for copy in head:
        copy.wait()
    first = {}
    for c in range(len(s.ff_chunks)):
        cols = body.columns(s.ff_chunks[c])
        for i, name in enumerate(("gate1", "up1")):
            first[c, i] = body.local(hbm[name].at[:, cols], r["v_" + name].at[:, cols], r["w1"].at[i, c])
    pl.semaphore_wait(sem, s.n + s.nt - 2)
    if not s.split:
        for d in range(1, s.nt):
            k = lax.rem(body.tp + d, s.nt)
            body.send(gains.at[body.tp], gains.at[body.tp], "n", tp=k)
        parts = sorted(range(s.parts), key=lambda part: part != ORDER[0] // 10000)
        for part in parts:
            block = r["feat"].at[:, part, :, mine]
            for d in range(1, s.nt):
                k = lax.rem(body.tp + d, s.nt)
                sent.append(copy_to(block, block, r["sent"].at[0], r["f"].at[part], tp=k))
                sent[-1].start()
        body.came(gains.at[pl.ds(0, s.nt - 1)], "n")

    def arrive(part):
        if not s.split:
            place = r["feat"].at[:, part, :, pl.ds(0, (s.nt - 1) * width)]
            pltpu.make_async_copy(place, place, r["f"].at[part]).wait()
        rows = r["feat"][:, part].astype(F32)
        r["b" + str(part)][...] = rows.reshape(s.rows, s.depth).astype(BF16)

    rest = {}
    begun = set()

    def ready(c):
        if c in begun:
            return
        first[c, 0].wait()
        first[c, 1].wait()
        if not begun:
            for i, name in enumerate(order):
                if name not in ("gate1", "up1"):
                    rest[name] = body.local(hbm[name], r["v_" + name], r["w"].at[i])
        begun.add(c)

    waited = set()

    def need(*wanted):
        for name in wanted:
            if name not in waited:
                waited.add(name)
                rest[name].wait()

    for body in bodies:
        body.need, body.ready, body.outs, body.arrive = need, ready, outs, arrive
    for code in ORDER:
        bodies[code // 10000].event(code // 1000 % 10, code // 10 % 100, code % 10)
    for copy in sent:
        copy.wait_send()


def write_kernel(s, blocks, past_ref, fresh_ref, next_ref, state_ref, state_out, past_out, next_out, moved, sem):
    taps, count = past_ref.shape[1], past_ref.shape[0]
    step = count // blocks
    copies = [pltpu.make_async_copy(next_ref, next_out, sem.at[blocks])]
    for k in range(blocks):
        rows = pl.ds(k * step, step)
        copies.append(pltpu.make_async_copy(state_ref.at[rows], state_out.at[rows], sem.at[k]))
    for copy in copies:
        copy.start()

    def one(k, carry):
        for t in range(taps - 1):
            moved[k, t] = past_ref[k, t + 1]
        newest = [fresh_ref[g, pl.ds(k, 1), :] for g in range(s.groups)]
        moved[k, taps - 1] = jnp.concatenate(newest, axis=0).astype(BF16)
        return carry

    lax.fori_loop(0, count, one, 0)
    copies.append(pltpu.make_async_copy(moved, past_out, sem.at[blocks + 1]))
    copies[-1].start()
    for copy in copies:
        copy.wait()


def gathered(stream, gains):
    n = lax.axis_size(TP)
    features = lax.all_gather(stream, TP, axis=1, tiled=True)
    packed = lax.all_gather(jnp.stack(gains), TP, axis=1, tiled=True)
    return features, packed


def on_device(
    stream,
    ssm_state,
    conv_state,
    first_gain,
    first_gate,
    first_up,
    first_down,
    mix_gain,
    gate_in,
    value_in,
    write_in,
    read_in,
    step_in,
    conv_weight,
    step_bias,
    log_decay_rate,
    group_gain,
    out_weight,
    last_norm_gain,
    second_gate,
    second_up,
    second_down,
):
    n, nt = lax.axis_size(KV), lax.axis_size(TP)
    rows, width = stream.shape
    depth, units = first_gate.shape
    heads, head, state = ssm_state.shape[1:]
    groups = conv_weight.shape[1]
    split = width % LANES != 0
    s = Sizes(n, nt, rows, depth, units, heads, head, state, groups, split)
    if split:
        features, packed = gathered(stream, [first_gain, mix_gain, last_norm_gain])
        named = {"stream": features.reshape(n, s.parts, s.count, depth), "gain1": packed}
    else:
        named = {
            "stream": stream.reshape(n, s.parts, s.count, width),
            "gain1": first_gain[None],
            "gain2": mix_gain[None],
            "gain3": last_norm_gain[None],
        }
    weights = {
        "gate1": first_gate,
        "up1": first_up,
        "down1": first_down,
        "value": value_in,
        "gate": gate_in,
        "write": write_in,
        "read": read_in,
        "step": step_in.T,
        "cw": conv_weight,
        "bias": step_bias[None],
        "rate": log_decay_rate[None],
        "gg": group_gain[None],
        "past": conv_state,
        "state": ssm_state,
        "out": out_weight,
        "gate2": second_gate,
        "up2": second_up,
        "down2": second_down,
    }
    plan = make_plan(s, [(k, v.shape, v.dtype) for k, v in weights.items()])
    named.update(weights)
    result, fresh, held = pl.pallas_call(
        functools.partial(step_kernel, s, plan, list(named)),
        out_shape=[
            pltpu.VMEM((n, s.parts, s.count, depth if split else width), BF16),
            pltpu.VMEM((groups, rows // n, s.channels), F32),
            pltpu.VMEM(ssm_state.shape, ssm_state.dtype),
        ],
        in_specs=[HB] * len(named),
        out_specs=[VM] * 3,
        scratch_shapes=plan.shapes,
        compiler_params=pltpu.CompilerParams(
            collective_id=0, has_side_effects=True, vmem_limit_bytes=48 * 1024 * 1024
        ),
    )(*named.values())
    if split:
        me = lax.axis_index(TP)
        result = lax.dynamic_slice_in_dim(result, me * width, width, axis=3)
    blocks = 8
    state_next, past_next, stream_next = pl.pallas_call(
        functools.partial(write_kernel, s, blocks),
        out_shape=[
            jax.ShapeDtypeStruct(ssm_state.shape, ssm_state.dtype),
            jax.ShapeDtypeStruct(conv_state.shape, conv_state.dtype),
            jax.ShapeDtypeStruct(result.shape, BF16),
        ],
        in_specs=[VM] * 4,
        out_specs=[HB] * 3,
        scratch_shapes=[pltpu.VMEM(conv_state.shape, BF16), pltpu.SemaphoreType.DMA((blocks + 2,))],
        compiler_params=pltpu.CompilerParams(vmem_limit_bytes=8 * 1024 * 1024),
    )(conv_state, fresh, result, held)
    return (stream_next.reshape(stream.shape), state_next, past_next)


def solution(mesh):
    return jax.shard_map(
        on_device,
        mesh=mesh,
        in_specs=(
            P(None, (KV, TP)),
            P(KV, TP, None, None),
            P(KV, None, TP, None),
            P((KV, TP)),
            P(KV, TP),
            P(KV, TP),
            P(TP, KV),
            P((KV, TP)),
            P(KV, TP),
            P(KV, TP),
            P(KV, TP),
            P(KV, TP),
            P(KV, TP),
            P(None, TP, None),
            P(TP),
            P(TP),
            P(TP),
            P(TP, KV),
            P((KV, TP)),
            P(KV, TP),
            P(KV, TP),
            P(TP, KV),
        ),
        out_specs=(P(None, (KV, TP)), P(KV, TP, None, None), P(KV, None, TP, None)),
        check_vma=False,
    )
```
